256 devices in a mesh: grp: 2 (over y), ep: 64 (over z, x), tp: 2 (over core).
Axes of the slice: x: 4, y: 2, z: 16, core: 2. Of those that a mesh axis runs over, the one named last changes fastest.
The devices are a block of a 4x16x16 slice.
Arguments:
- tokens: bfloat16 [65536, 2048], P(('grp', 'ep', 'tp')), parts along dimension 0, may hold values from -15 to 15
- gain_in: float32 [2048], replicated, may hold values from 0.1 to 1.9
- expert_ids: int32 [65536, 2], P(('grp', 'ep')), parts along dimension 0, may hold values from 0 to 63, all different within a row; in each aligned block of 256 rows (0 to 255, 256 to 511, ...) at most 16 rows name the same one
- gate_weights: float32 [65536, 2], P(('grp', 'ep')), parts along dimension 0, may hold values from 0.1 to 1
- w_gate: bfloat16 [64, 2048, 512], P('ep', None, 'tp'), may hold values from -0.125 to 0.125
- w_up: bfloat16 [64, 2048, 512], P('ep', None, 'tp'), may hold values from -0.125 to 0.125
- w_down: bfloat16 [64, 2048, 512], P('ep', None, 'tp'), may hold values from -20 to 20
- gain_out: float32 [2048], P('tp'), may hold values from 0.1 to 1.9
Outputs:
- mixed: bfloat16 [65536, 2048], P(('grp', 'ep'), 'tp'), parts along dimension 0
The draws below stay inside these ranges and needn't reach their ends.
There are 2 independent parts, one for each index of `grp`. The reference program is written for one: setup_inputs(seed, part) draws one part's arguments, and reference() takes and returns one part's arrays. A program takes and returns all parts, laid end to end along the dimension named above; an argument that names none is the same for every part. Nothing has to cross between parts.
Inputs may be any that keep to these rules, and one draw needn't show every extreme that they name: `expert_ids`: each token names 2 different experts; in each aligned block of 256 tokens no expert is named by more than 16 pairs, a bound that some block reaches.
All inputs are finite; a program needn't handle non-finite values.
Results may differ from the reference program's by a relative error of at most 0.0077.
Values may be sent and summed in bfloat16 or wider, within the bound.
A program may use at most 64 MiB of HBM per device.

```python
import math
import jax
import jax.numpy as jnp
import numpy as np
from jax import lax

D = 2048
DE = 512
TOP_K = 2
TOK_DEV = 256
EXPERTS = 64
CAP = 16
HALVES = 2
TOKENS = 32768


def draw_w_down(key, part):
    jitter = jax.random.uniform(jax.random.fold_in(key, 12), (D,), jnp.float32, 0.6, 1.4)
    column = jnp.arange(D, dtype=jnp.float32) / D
    base = jnp.clip(jax.random.normal(jax.random.fold_in(key, 11), (EXPERTS, D, DE), jnp.float32), -4.0, 4.0)
    rise = 10.0 ** column
    values = base * (rise * jitter)[None, :, None] * DE ** (-0.5)
    return jnp.clip(values, -20.0, 20.0).astype(jnp.bfloat16)


def block_levels(rng, shape, pieces, smallest, top_value):
    gain = 1.0
    for dim, blocks in pieces:
        steps = jax.random.uniform(jax.random.fold_in(jax.random.fold_in(rng, 6), dim), (blocks,), jnp.float32, smallest / len(pieces), top_value / len(pieces))
        gain = gain * jnp.repeat(jnp.exp(steps), shape[dim] // blocks).reshape((-1,) + (1,) * (len(shape) - 1 - dim))
    return gain


def assign_block(stream_key, own, number, rows, number_of, top, reach, slope):
    sequence = jax.random.permutation(stream_key, number_of)
    heavy_load, ordinary = shares(number_of, rows * top, reach, slope, True), shares(number_of, rows * top, reach, slope, False)
    places = jnp.arange(number_of)

    def named(sizes, offset_by):
        used = int((sizes > 0).sum())
        fixed = max(1, used // 4)
        moved = fixed + (places - fixed + offset_by * (used - fixed)) % max(1, number_of - fixed)
        return jnp.zeros((number_of,), jnp.int32).at[sequence[jnp.where(places < fixed, places, moved)]].set(jnp.asarray(sizes, jnp.int32))

    sizes = jnp.where(number % 4 == 0, named(heavy_load, number // 4), named(ordinary, number - number // 4 - 1))
    mixed = jax.random.permutation(jax.random.fold_in(own, 3), number_of)
    source_of, receiver = mixed[0:number_of // 2 * 2:2], mixed[1:number_of // 2 * 2:2]
    room = jnp.minimum(sizes[source_of] - 1, reach - sizes[receiver]) // 2
    room = jnp.where((source_of == sequence[0]) | (receiver == sequence[0]) | (sizes[receiver] == 0), 0, jnp.maximum(room, 0))
    moved = jax.random.randint(jax.random.fold_in(own, 4), (number_of // 2,), 0, 1 << 20) % (room + 1)
    sizes = sizes.at[source_of].add(-moved).at[receiver].add(moved)
    items = jnp.searchsorted(jnp.cumsum(sizes), jnp.arange(rows * top), side="right").astype(jnp.int32)
    table = items.reshape(top, rows).T
    table = table[jax.random.permutation(jax.random.fold_in(own, 1), rows)]
    offset_by = jax.random.randint(jax.random.fold_in(own, 2), (rows, 1), 0, top)
    return jnp.take_along_axis(table, (jnp.arange(top)[None, :] + offset_by) % top, axis=1)


def shares(amount, total, most, lean, full):
    portions = [(1 << 20) // math.isqrt(grade ** lean) + 1 for grade in range(1, amount + 1)]
    largest = most if full else min(most, max(-(-total // amount), total * portions[0] // sum(portions)))
    least = 1 if total - largest >= amount - 1 else 0
    given, spare = [largest] + [least] * (amount - 1), total - largest - least * (amount - 1)
    while spare > 0:
        movable = [i for i in range(1, amount) if given[i] < largest] or [i for i in range(1, amount) if given[i] < most]
        whole, left = sum([portions[i] for i in movable]), spare
        for i in movable:
            addition = min(most - given[i], max(1, left * portions[i] // whole), spare)
            given[i] = given[i] + addition
            spare = spare - addition
    return np.array(given)


def gaussian(rng, dims, spread, most, shards=(), kind=jnp.bfloat16):
    result = jax.random.normal(rng, dims, jnp.float32) * spread
    if len(shards) > 0:
        result = block_levels(rng, dims, shards, -0.22, 0.18) * result
    return jnp.clip(result, min=-most, max=most).astype(kind)


def setup_inputs(seed: int = 0, part: int = 0) -> dict:
    seeds = jax.random.split(jax.random.key(seed), 9)
    part_splits = jax.random.split(jax.random.fold_in(seeds[8], part), 9)
    tokens = gaussian(part_splits[0], (TOKENS, D), 3.0, 15.0, ((0, 128),))
    gain_in = jnp.clip(1.0 + 0.18 * jax.random.normal(seeds[1], (D,), jnp.float32), 0.1, 1.9)
    expert_ids_keys = jax.random.split(jax.random.fold_in(part_splits[2], 1), TOKENS // TOK_DEV)
    expert_ids_turns = jax.random.permutation(jax.random.fold_in(part_splits[2], 3), TOKENS // TOK_DEV)
    expert_ids = jax.vmap(lambda own, number: assign_block(jax.random.fold_in(part_splits[2], 2), own, number, TOK_DEV, EXPERTS, TOP_K, CAP, 2))(expert_ids_keys, expert_ids_turns).reshape((TOKENS, TOP_K))
    gate_weights = jnp.clip(jnp.exp(math.log(1.0) - 2.3025851 * jax.random.uniform(part_splits[3], (TOKENS, TOP_K), jnp.float32) ** block_levels(part_splits[3], (TOKENS, TOP_K), ((0, 64),), -0.2, 0.2)), 0.1, 1.0)
    w_gate = gaussian(seeds[4], (EXPERTS, D, DE), D ** -0.5, 0.125, ((0, 64), (2, 2)))
    w_up = gaussian(seeds[5], (EXPERTS, D, DE), D ** -0.5, 0.125, ((0, 64), (2, 2)))
    w_down = draw_w_down(jax.random.fold_in(seeds[8], 71), part)
    gain_out = jnp.clip(1.0 + 0.18 * jax.random.normal(seeds[7], (D,), jnp.float32), 0.1, 1.9)
    return dict(tokens=tokens, gain_in=gain_in, expert_ids=expert_ids, gate_weights=gate_weights, w_gate=w_gate, w_up=w_up, w_down=w_down, gain_out=gain_out)


EPS = 1e-06

def block_slots(expert_ids, block_rows, experts):
    pairs = expert_ids.reshape(-1, block_rows * expert_ids.shape[1])
    onehot = (pairs[:, :, None] == jnp.arange(experts, dtype=jnp.int32)[None, None, :]).astype(jnp.int32)
    before = jnp.cumsum(onehot, axis=1) - onehot
    return lax.optimization_barrier(jnp.sum(before * onehot, axis=2)).reshape(expert_ids.shape).astype(jnp.int32)

def reference(tokens, gain_in, expert_ids, gate_weights, w_gate, w_up, w_down, gain_out):
    x_float = tokens.astype(jnp.float32)
    normed = (x_float * lax.rsqrt(lax.optimization_barrier(jnp.mean(x_float * x_float, axis=1, keepdims=True)) + EPS) * gain_in).astype(jnp.bfloat16)
    slots = block_slots(expert_ids, TOK_DEV, EXPERTS)
    sources = TOKENS // TOK_DEV
    token_ids = jnp.broadcast_to(jnp.arange(TOKENS, dtype=jnp.int32)[:, None], expert_ids.shape)
    position = token_ids // TOK_DEV * CAP + slots
    table = jnp.full((EXPERTS, sources * CAP), TOKENS, jnp.int32).at[expert_ids, position].set(token_ids)
    row_gates = jnp.zeros((EXPERTS, sources * CAP), jnp.float32).at[expert_ids, position].set(gate_weights)
    padded = jnp.concatenate([normed, jnp.zeros((1, D), jnp.bfloat16)], axis=0)
    block = DE // HALVES

    def one_expert(total, inputs):
        rows_index, gates_here, gate_matrix, up_matrix, down_matrix = inputs
        rows = padded[rows_index]
        gated = jnp.dot(rows, gate_matrix, preferred_element_type=jnp.float32)
        upward = jnp.dot(rows, up_matrix, preferred_element_type=jnp.float32)
        hidden = (jax.nn.silu(gated) * upward).astype(jnp.bfloat16)
        summed = jnp.zeros((rows.shape[0], D), jnp.float32)
        for index in range(HALVES):
            part = lax.dot_general(hidden[:, index * block:(index + 1) * block], down_matrix[:, index * block:(index + 1) * block], (((1,), (1,)), ((), ())), preferred_element_type=jnp.float32)
            summed = summed + lax.optimization_barrier(part.astype(jnp.bfloat16)).astype(jnp.float32)
        expert_out = summed.astype(jnp.bfloat16).astype(jnp.float32)
        return (total.at[rows_index].add(gates_here[:, None] * expert_out), None)
    combined, _ = lax.scan(one_expert, jnp.zeros((TOKENS + 1, D), jnp.float32), (table, row_gates, w_gate, w_up, w_down))
    combined = combined[:TOKENS]
    inverse = lax.rsqrt(lax.optimization_barrier(jnp.mean(combined * combined, axis=1, keepdims=True)) + EPS)
    return (combined * inverse * gain_out).astype(jnp.bfloat16)
```

```python
import functools

import jax
import jax.numpy as jnp
from jax import lax
from jax.experimental import pallas as pl
from jax.experimental.pallas import tpu as pltpu
from jax.sharding import PartitionSpec as P

EPS = 1e-06
COLUMNS = 4
MESH = pl.DeviceIdType.MESH
VMEM = pl.BlockSpec(memory_space=pltpu.VMEM)
ANY = pl.BlockSpec(memory_space=pl.ANY)
VMEM_LIMIT = 60 * 1024 * 1024


class Plan:
    def __init__(self, rows, width, members, capacity, columns):
        self.rows, self.width, self.members, self.cap, self.X = rows, width, members, capacity, columns
        self.Z = members // columns
        self.H = self.Z // 2
        self.slots = columns * capacity
        self.piece = self.slots // 2
        self.prefix = [0] + [
            min(rows, (self.H - d) * self.slots + self.slots // 2) for d in range(1, self.H + 1)
        ] + [0]
        self.pieces = [n // self.piece for n in self.prefix]
        self.offset = [sum(self.prefix[:d]) for d in range(self.H + 2)]
        self.total = sum(self.prefix)
        self.most = max(self.pieces)

    def me(self):
        ep = lax.axis_index("ep")
        return ep // self.X, ep % self.X

    def at(self, z, x):
        return lax.rem(z + 2 * self.Z, self.Z) * self.X + lax.rem(x + 2 * self.X, self.X)


def remote(src, dst, send, recv, **where):
    return pltpu.make_async_remote_copy(
        src_ref=src, dst_ref=dst, send_sem=send, recv_sem=recv, device_id=where, device_id_type=MESH
    )


def greet(plan, partner):
    z, x = plan.me()
    barrier = pltpu.get_barrier_semaphore()
    peers = [{"ep": plan.at(z + 1, x)}, {"ep": plan.at(z - 1, x)}]
    peers += [{"ep": plan.at(z, x + r)} for r in range(1, plan.X)]
    if partner:
        peers.append({"tp": 1 - lax.axis_index("tp")})
    for peer in peers:
        pl.semaphore_signal(barrier, inc=1, device_id=peer, device_id_type=MESH)
    pl.semaphore_wait(barrier, len(peers))


def iota(shape, dim):
    return lax.broadcasted_iota(jnp.int32, shape, dim)


def sort_kernel(plan, x_ref, gain_ref, ids_ref, gates_ref, plus_ref, minus_ref, meta_ref, normed):
    rows, X, Z, H = plan.rows, plan.X, plan.Z, plan.H
    z, _ = plan.me()
    step = 32

    def norm_step(i, carry):
        here = pl.ds(pl.multiple_of(i * step, step), step)
        x = x_ref[here, :].astype(jnp.float32)
        scale = lax.rsqrt(jnp.mean(x * x, axis=1, keepdims=True) + EPS)
        normed[here, :] = (x * scale * gain_ref[...]).astype(jnp.bfloat16)
        return carry

    lax.fori_loop(0, rows // step, norm_step, 0)

    own = pl.ds(pl.multiple_of(lax.axis_index("tp") * rows, rows), rows)
    ids, gates = ids_ref[own, :], gates_ref[own, :]
    square = (rows, rows)
    sub, lane = iota(square, 0), iota(square, 1)
    eye = sub == lane

    def as_row(column):
        return jnp.sum(jnp.where(eye, column, 0.0), axis=0, keepdims=True)

    def count(mask, axis):
        return jnp.sum(jnp.where(mask, 1.0, 0.0), axis=axis, keepdims=True)

    cols = [ids[:, k : k + 1].astype(jnp.float32) for k in range(2)]
    rws = [as_row(c) for c in cols]
    gcols = [gates[:, k : k + 1] for k in range(2)]
    grws = [as_row(g) for g in gcols]
    q_col, q_row, key_col, key_row = [], [], [[], []], [[], []]
    for k in range(2):
        slot_row = count((sub < lane) & (cols[0] == rws[k]), 0) + count((sub < lane) & (cols[1] == rws[k]), 0)
        slot_col = count((lane < sub) & (rws[0] == cols[k]), 1) + count((lane < sub) & (rws[1] == cols[k]), 1)
        q_row.append(rws[k] * plan.cap + slot_row)
        q_col.append(cols[k] * plan.cap + slot_col)
        for expert, keys in ((rws[k], key_row), (cols[k], key_col)):
            e = expert.astype(jnp.int32)
            ahead = e // X - z
            ahead = jnp.where(ahead < 0, ahead + Z, ahead)
            first = e % X < X // 2
            up = jnp.where((ahead < H) | ((ahead == H) & first), ahead, 0)
            down = jnp.where((ahead > H) | ((ahead == H) & ~first), Z - ahead, 0)
            keys[0].append(up.astype(jnp.float32))
            keys[1].append(down.astype(jnp.float32))
    for k in range(2):
        meta_ref[2, k : k + 1, :] = q_row[k]
        meta_ref[2, 2 + k : 3 + k, :] = grws[k]
    for way, out in ((0, plus_ref), (1, minus_ref)):
        far_col = jnp.maximum(*key_col[way])
        far_row = jnp.maximum(*key_row[way])
        rank_row = count((far_col > far_row) | ((far_col == far_row) & (sub < lane)), 0)
        rank_col = count((far_row > far_col) | ((far_row == far_col) & (lane < sub)), 1)
        meta_ref[2, 4 + way : 5 + way, :] = rank_row
        chosen = rank_col == lane.astype(jnp.float32)
        for k in range(2):
            meta_ref[way, k : k + 1, :] = jnp.sum(jnp.where(chosen, q_col[k], 0.0), axis=0, keepdims=True)
            meta_ref[way, 2 + k : 3 + k, :] = jnp.sum(jnp.where(chosen, gcols[k], 0.0), axis=0, keepdims=True)
        meta_ref[way, 4:8, :] = jnp.zeros((4, rows), jnp.float32)
        order = jnp.where(sub.astype(jnp.float32) == rank_row, 1.0, 0.0).astype(jnp.bfloat16)
        for c in range(0, plan.width, 512):
            n = min(512, plan.width)
            out[:, c : c + n] = jnp.dot(
                order, normed[:, c : c + n], preferred_element_type=jnp.float32
            ).astype(jnp.bfloat16)
    meta_ref[2, 6:8, :] = jnp.zeros((2, rows), jnp.float32)


def sort_tokens(plan, tokens, gain_in, expert_ids, gate_weights):
    rows, width = plan.rows, plan.width
    return pl.pallas_call(
        functools.partial(sort_kernel, plan),
        out_shape=(
            jax.ShapeDtypeStruct((rows, width), jnp.bfloat16),
            jax.ShapeDtypeStruct((rows, width), jnp.bfloat16),
            jax.ShapeDtypeStruct((3, 8, rows), jnp.float32),
        ),
        in_specs=[VMEM] * 4,
        out_specs=(VMEM,) * 3,
        scratch_shapes=[pltpu.VMEM((rows, width), jnp.bfloat16)],
        compiler_params=pltpu.CompilerParams(vmem_limit_bytes=VMEM_LIMIT),
        name="sort_tokens",
    )(tokens, gain_in.reshape(1, width), expert_ids, gate_weights)


def hits(plan, meta, n, z, way, d, weighted):
    slots, cap = plan.slots, plan.cap
    slot = iota((slots, n), 0)
    base = z * slots
    total = jnp.zeros((slots, n), jnp.float32)
    for k in range(2):
        match = meta[k : k + 1, :n].astype(jnp.int32) - base == slot
        if d == plan.H:
            match = match & (slot < slots // 2 if way == 0 else slot >= slots // 2)
        total = total + jnp.where(match, meta[2 + k : 3 + k, :n] if weighted else 1.0, 0.0)
    return total


def dispatch_kernel(
    plan,
    plus_ref, minus_ref, meta_ref, wg_ref, wu_ref, wd_ref,
    arrived_ref, og_ref, ou_ref, od_ref, metas_ref,
    ring, metas, stage, zsend, zrecv, msend, mrecv, xsend, xrecv, lsem, wsend, wrecv,
):
    X, Z, H, cap, piece = plan.X, plan.Z, plan.H, plan.cap, plan.piece
    z, x = plan.me()
    greet(plan, True)
    other = 1 - lax.axis_index("tp")

    own = (plus_ref, minus_ref)
    ahead = (plan.at(z + 1, x), plan.at(z - 1, x))

    def passing(way, d, p):
        dst = ring.at[way, pl.ds(plan.offset[d] + p * piece, piece), :]
        if d == 1:
            src = own[way].at[pl.ds(p * piece, piece), :]
        else:
            src = ring.at[way, pl.ds(plan.offset[d - 1] + p * piece, piece), :]
        return remote(src, dst, zsend.at[way, d - 1, p], zrecv.at[way, d - 1, p], ep=ahead[way])

    def passing_meta(way, d):
        src = meta_ref.at[way] if d == 1 else metas.at[way, d - 2]
        return remote(src, metas.at[way, d - 1], msend.at[way, d - 1], mrecv.at[way, d - 1], ep=ahead[way])

    def hand_over(k, r):
        column = lax.rem(x + r, X)
        src = stage.at[k, pl.ds(pl.multiple_of(column * cap, cap), cap), :]
        block = pl.multiple_of(plan.at(z + k, x) * cap, cap)
        dst = arrived_ref.at[pl.ds(block, cap), :]
        if r == 0:
            return pltpu.make_async_copy(src, dst, lsem.at[k])
        return remote(src, dst, xsend.at[k, r], xrecv.at[k, r], ep=plan.at(z, x + r))

    def pick(source, meta, n, way, d, k):
        chosen = hits(plan, meta, n, z, way, d, False).astype(jnp.bfloat16)
        wide = min(512, plan.width)

        def columns(c, carry):
            here = pl.ds(pl.multiple_of(c * wide, wide), wide)
            found = jnp.dot(chosen, source[:n, here], preferred_element_type=jnp.float32)
            found = found.astype(jnp.bfloat16)
            if d == H:
                half = plan.slots // 2
                lo = 0 if way == 0 else half
                stage[k, lo : lo + half, here] = found[lo : lo + half, :]
            else:
                stage[k, :, here] = found
            return carry

        lax.fori_loop(0, plan.width // wide, columns, 0)

    for way in range(2):
        passing_meta(way, 1).start()
    for p in range(plan.pieces[1]):
        for way in range(2):
            passing(way, 1, p).start()
    weights = [
        remote(src, dst, wsend.at[i], wrecv.at[i], tp=other)
        for i, (src, dst) in enumerate(((wg_ref, og_ref), (wu_ref, ou_ref), (wd_ref, od_ref)))
    ]
    for copy in weights:
        copy.start()

    def send_rows(k):
        for r in range(1, X):
            hand_over(k, r).start()
        hand_over(k, 0).start()

    pick(plus_ref, meta_ref[0], plan.rows, 0, 0, 0)
    ready = [0]
    for d in range(1, H + 1):
        for way in range(2):
            passing_meta(way, d).wait_recv()
            if d < H:
                passing_meta(way, d + 1).start()
        for p in range(plan.pieces[d]):
            for way in range(2):
                passing(way, d, p).wait_recv()
                if p < plan.pieces[d + 1]:
                    passing(way, d + 1, p).start()
        for k in ready:
            send_rows(k)
        ready = []
        for way in range(2):
            k = (Z - d if way == 0 else d) % Z
            n = plan.prefix[d]
            pick(ring.at[way, pl.ds(plan.offset[d], n), :], metas[way, d - 1], n, way, d, k)
            if d < H:
                ready.append(k)
    metas_ref[...] = metas[...]
    for k in [H] + ready:
        send_rows(k)

    for k in range(Z):
        for r in range(1, X):
            hand_over(k, r).wait_recv()
        hand_over(k, 0).wait()
    for copy in weights:
        copy.wait()
    for k in range(Z):
        for r in range(1, X):
            hand_over(k, r).wait_send()
    for d in range(1, H + 1):
        for way in range(2):
            passing_meta(way, d).wait_send()
            for p in range(plan.pieces[d]):
                passing(way, d, p).wait_send()


def dispatch(plan, plus, minus, meta, w_gate, w_up, w_down):
    X, Z, H, rows, width = plan.X, plan.Z, plan.H, plan.rows, plan.width
    dma = pltpu.SemaphoreType.DMA
    return pl.pallas_call(
        functools.partial(dispatch_kernel, plan),
        out_shape=(
            jax.ShapeDtypeStruct((plan.members * plan.cap, width), jnp.bfloat16),
            jax.ShapeDtypeStruct(w_gate.shape, w_gate.dtype),
            jax.ShapeDtypeStruct(w_up.shape, w_up.dtype),
            jax.ShapeDtypeStruct(w_down.shape, w_down.dtype),
            jax.ShapeDtypeStruct((2, H, 8, rows), jnp.float32),
        ),
        in_specs=[VMEM, VMEM, VMEM, ANY, ANY, ANY],
        out_specs=(ANY, ANY, ANY, ANY, VMEM),
        scratch_shapes=[
            pltpu.VMEM((2, plan.total, width), jnp.bfloat16),
            pltpu.VMEM((2, H, 8, rows), jnp.float32),
            pltpu.VMEM((Z, plan.slots, width), jnp.bfloat16),
            dma((2, H, plan.most)), dma((2, H, plan.most)), dma((2, H)), dma((2, H)),
            dma((Z, X)), dma((Z, X)), dma((Z,)), dma((3,)), dma((3,)),
        ],
        compiler_params=pltpu.CompilerParams(
            collective_id=0, has_side_effects=True, vmem_limit_bytes=VMEM_LIMIT
        ),
        name="dispatch",
    )(plus, minus, meta, w_gate, w_up, w_down)


def combine_kernel(
    plan,
    out_ref, meta_ref, metas_ref,
    scaled_ref,
    back, leaving, rows_in, spread, doubled, zsend, zrecv, xsend, xrecv, lsem,
):
    X, Z, H, cap, piece, width = plan.X, plan.Z, plan.H, plan.cap, plan.piece, plan.width
    z, x = plan.me()
    greet(plan, False)
    ahead = (plan.at(z - 1, x), plan.at(z + 1, x))
    wide = min(512, width)

    def give_back(k, r):
        block = pl.multiple_of(plan.at(z + k, x + r) * cap, cap)
        dst = rows_in.at[k, pl.ds(pl.multiple_of(x * cap, cap), cap), :]
        src = out_ref.at[pl.ds(block, cap), :]
        if r == 0:
            return pltpu.make_async_copy(src, dst, lsem.at[k])
        return remote(src, dst, xsend.at[k, r], xrecv.at[k, r], ep=plan.at(z, x + r))

    def passing(way, d, p):
        here = pl.ds(plan.offset[d] + p * piece, piece)
        return remote(
            leaving.at[way, here, :], back.at[way, here, :],
            zsend.at[way, d - 1, p], zrecv.at[way, d - 1, p], ep=ahead[way],
        )

    def sources(d):
        return sorted({(Z - d) % Z, d % Z})

    for d in range(H, -1, -1):
        for k in sources(d):
            for r in range(X):
                give_back(k, r).start()

    def prepare(way, d, k, meta, n):
        w = hits(plan, meta, n, z, way, d, True)
        high = w.astype(jnp.bfloat16).astype(jnp.float32)
        both = jnp.concatenate([high, w - high], axis=0)
        spread[way, :n, :] = both.T.astype(jnp.bfloat16)
        doubled[way, : plan.slots, :] = rows_in[k]
        doubled[way, plan.slots :, :] = rows_in[k]

    def wait_rows(k):
        for r in range(1, X):
            give_back(k, r).wait_recv()
        give_back(k, 0).wait()

    for d in range(H, 0, -1):
        for k in sources(d):
            wait_rows(k)
        for way in range(2):
            prepare(way, d, (Z - d if way == 0 else d) % Z, metas_ref[way, d - 1], plan.prefix[d])

        def one(p, carry, joined, d=d):
            for way in range(2):
                if joined:
                    passing(way, d + 1, p).wait_recv()
                place = spread[way, pl.ds(pl.multiple_of(p * piece, piece), piece), :]
                mine = pl.ds(pl.multiple_of(plan.offset[d] + p * piece, piece), piece)
                for c in range(0, width, wide):
                    part = jnp.dot(
                        place, doubled[way, :, c : c + wide], preferred_element_type=jnp.float32
                    )
                    if joined:
                        there = pl.ds(pl.multiple_of(plan.offset[d + 1] + p * piece, piece), piece)
                        part = part + back[way, there, c : c + wide].astype(jnp.float32)
                    leaving[way, mine, c : c + wide] = part.astype(jnp.bfloat16)
            for way in range(2):
                passing(way, d, p).start()
            return carry

        old, new = plan.pieces[d + 1], plan.pieces[d]
        if new > old:
            lax.fori_loop(old, new, functools.partial(one, joined=False), 0)
        if old:
            lax.fori_loop(0, old, functools.partial(one, joined=True), 0)

    wait_rows(0)
    prepare(0, 0, 0, meta_ref[2], plan.rows)
    for way in range(2):
        def arrive(p, carry, way=way):
            passing(way, 1, p).wait_recv()
            return carry

        lax.fori_loop(0, plan.pieces[1], arrive, 0)
    ranks = meta_ref[2]
    order = []
    for way in range(2):
        slot = iota((plan.rows, plan.rows), 0).astype(jnp.float32)
        order.append(jnp.where(slot == ranks[4 + way : 5 + way, :], 1.0, 0.0).T.astype(jnp.bfloat16))
    total = jnp.zeros((plan.rows, 1), jnp.float32)
    first = plan.offset[1]
    sums = []
    for c in range(0, width, wide):
        part = jnp.dot(spread[0], doubled[0, :, c : c + wide], preferred_element_type=jnp.float32)
        for way in range(2):
            part = part + jnp.dot(
                order[way], back[way, first : first + plan.rows, c : c + wide],
                preferred_element_type=jnp.float32,
            )
        sums.append(part)
        total = total + jnp.sum(part * part, axis=1, keepdims=True)
    inverse = lax.rsqrt(total / width + EPS)
    for i, c in enumerate(range(0, width, wide)):
        scaled_ref[:, c : c + wide] = (sums[i] * inverse).astype(jnp.bfloat16)

    for k in range(Z):
        for r in range(1, X):
            give_back(k, r).wait_send()
    for d in range(1, H + 1):
        for way in range(2):
            def gone(p, carry, way=way, d=d):
                passing(way, d, p).wait_send()
                return carry

            lax.fori_loop(0, plan.pieces[d], gone, 0)


def combine(plan, out, meta, metas):
    X, Z, H, rows, width = plan.X, plan.Z, plan.H, plan.rows, plan.width
    dma = pltpu.SemaphoreType.DMA
    return pl.pallas_call(
        functools.partial(combine_kernel, plan),
        out_shape=jax.ShapeDtypeStruct((rows, width), jnp.bfloat16),
        in_specs=[ANY, VMEM, VMEM],
        out_specs=VMEM,
        scratch_shapes=[
            pltpu.VMEM((2, plan.total, width), jnp.bfloat16),
            pltpu.VMEM((2, plan.total, width), jnp.bfloat16),
            pltpu.VMEM((Z, plan.slots, width), jnp.bfloat16),
            pltpu.VMEM((2, rows, 2 * plan.slots), jnp.bfloat16),
            pltpu.VMEM((2, 2 * plan.slots, width), jnp.bfloat16),
            dma((2, H, plan.most)), dma((2, H, plan.most)),
            dma((Z, X)), dma((Z, X)), dma((Z,)),
        ],
        compiler_params=pltpu.CompilerParams(
            collective_id=1, has_side_effects=True, vmem_limit_bytes=VMEM_LIMIT
        ),
        name="combine",
    )(out, meta, metas)


def expert_half(rows, gate_matrix, up_matrix, down_matrix):
    gated = jnp.dot(rows, gate_matrix, preferred_element_type=jnp.float32)
    upward = jnp.dot(rows, up_matrix, preferred_element_type=jnp.float32)
    hidden = (jax.nn.silu(gated) * upward).astype(jnp.bfloat16)
    part = lax.dot_general(
        hidden, down_matrix, (((1,), (1,)), ((), ())), preferred_element_type=jnp.float32
    )
    return lax.optimization_barrier(part.astype(jnp.bfloat16)).astype(jnp.float32)


def per_device(columns, tokens, gain_in, expert_ids, gate_weights, w_gate, w_up, w_down, gain_out):
    own_rows, width = tokens.shape
    members = lax.axis_size("ep")
    capacity = 2 * own_rows * expert_ids.shape[1] // members
    plan = Plan(own_rows, width, members, capacity, columns)
    plus, minus, meta = sort_tokens(plan, tokens, gain_in, expert_ids, gate_weights)
    arrived, o_gate, o_up, o_down, metas = dispatch(
        plan, plus, minus, meta, w_gate[0], w_up[0], w_down[0]
    )
    summed = expert_half(arrived, w_gate[0], w_up[0], w_down[0])
    summed = summed + expert_half(arrived, o_gate, o_up, o_down)
    scaled = combine(plan, summed.astype(jnp.bfloat16), meta, metas)
    scaled = lax.all_to_all(scaled, "tp", split_axis=1, concat_axis=0, tiled=True)
    return (scaled.astype(jnp.float32) * gain_out).astype(jnp.bfloat16)


def solution(mesh, columns=COLUMNS):
    placed = (
        P(("grp", "ep", "tp"), None),
        P(),
        P(("grp", "ep"), None),
        P(("grp", "ep"), None),
        P("ep", None, "tp"),
        P("ep", None, "tp"),
        P("ep", None, "tp"),
        P("tp"),
    )
    return jax.shard_map(
        functools.partial(per_device, columns),
        mesh=mesh, in_specs=placed, out_specs=P(("grp", "ep"), "tp"), check_vma=False,
    )
```

```python
import functools

import jax
import jax.numpy as jnp
from jax import lax
from jax.experimental import pallas as pl
from jax.experimental.pallas import tpu as pltpu
from jax.sharding import PartitionSpec as P

EPS = 1e-06
COLUMNS = 4
MESH = pl.DeviceIdType.MESH
VMEM = pl.BlockSpec(memory_space=pltpu.VMEM)
ANY = pl.BlockSpec(memory_space=pl.ANY)
VMEM_LIMIT = 60 * 1024 * 1024


class Plan:
    def __init__(self, rows, width, members, capacity, columns):
        self.rows, self.width, self.members, self.cap, self.X = rows, width, members, capacity, columns
        self.Z = members // columns
        self.H = self.Z // 2
        self.slots = columns * capacity
        self.piece = self.slots // 2
        self.prefix = [0] + [
            min(rows, (self.H - d) * self.slots + self.slots // 2) for d in range(1, self.H + 1)
        ] + [0]
        self.pieces = [n // self.piece for n in self.prefix]
        self.offset = [sum(self.prefix[:d]) for d in range(self.H + 2)]
        self.total = sum(self.prefix)
        self.most = max(self.pieces)

    def me(self):
        ep = lax.axis_index("ep")
        return ep // self.X, ep % self.X

    def at(self, z, x):
        return lax.rem(z + 2 * self.Z, self.Z) * self.X + lax.rem(x + 2 * self.X, self.X)


def remote(src, dst, send, recv, **where):
    return pltpu.make_async_remote_copy(
        src_ref=src, dst_ref=dst, send_sem=send, recv_sem=recv, device_id=where, device_id_type=MESH
    )


def greet(plan, partner):
    z, x = plan.me()
    barrier = pltpu.get_barrier_semaphore()
    peers = [{"ep": plan.at(z + 1, x)}, {"ep": plan.at(z - 1, x)}]
    peers += [{"ep": plan.at(z, x + r)} for r in range(1, plan.X)]
    if partner:
        peers.append({"tp": 1 - lax.axis_index("tp")})
    for peer in peers:
        pl.semaphore_signal(barrier, inc=1, device_id=peer, device_id_type=MESH)
    pl.semaphore_wait(barrier, len(peers))


def iota(shape, dim):
    return lax.broadcasted_iota(jnp.int32, shape, dim)


def sort_kernel(plan, x_ref, gain_ref, ids_ref, gates_ref, plus_ref, minus_ref, meta_ref, normed):
    rows, X, Z, H = plan.rows, plan.X, plan.Z, plan.H
    z, _ = plan.me()
    step = 32

    def norm_step(i, carry):
        here = pl.ds(pl.multiple_of(i * step, step), step)
        x = x_ref[here, :].astype(jnp.float32)
        scale = lax.rsqrt(jnp.mean(x * x, axis=1, keepdims=True) + EPS)
        normed[here, :] = (x * scale * gain_ref[...]).astype(jnp.bfloat16)
        return carry

    lax.fori_loop(0, rows // step, norm_step, 0)

    own = pl.ds(pl.multiple_of(lax.axis_index("tp") * rows, rows), rows)
    square = (rows, rows)
    sub, lane = iota(square, 0), iota(square, 1)
    eye = sub == lane

    def as_column(row):
        return jnp.sum(jnp.where(eye, row, 0.0), axis=1, keepdims=True)

    def count(mask, axis):
        return jnp.sum(jnp.where(mask, 1.0, 0.0), axis=axis, keepdims=True)

    rws = [ids_ref[k : k + 1, own].astype(jnp.float32) for k in range(2)]
    cols = [as_column(r) for r in rws]
    grws = [gates_ref[k : k + 1, own] for k in range(2)]
    gcols = [as_column(g) for g in grws]
    q_col, q_row, key_col, key_row = [], [], [[], []], [[], []]
    for k in range(2):
        slot_row = count((sub < lane) & (cols[0] == rws[k]), 0) + count((sub < lane) & (cols[1] == rws[k]), 0)
        slot_col = count((lane < sub) & (rws[0] == cols[k]), 1) + count((lane < sub) & (rws[1] == cols[k]), 1)
        q_row.append(rws[k] * plan.cap + slot_row)
        q_col.append(cols[k] * plan.cap + slot_col)
        for expert, keys in ((rws[k], key_row), (cols[k], key_col)):
            e = expert.astype(jnp.int32)
            ahead = e // X - z
            ahead = jnp.where(ahead < 0, ahead + Z, ahead)
            first = e % X < X // 2
            up = jnp.where((ahead < H) | ((ahead == H) & first), ahead, 0)
            down = jnp.where((ahead > H) | ((ahead == H) & ~first), Z - ahead, 0)
            keys[0].append(up.astype(jnp.float32))
            keys[1].append(down.astype(jnp.float32))
    for k in range(2):
        meta_ref[2, k : k + 1, :] = q_row[k]
        meta_ref[2, 2 + k : 3 + k, :] = grws[k]
    for way, out in ((0, plus_ref), (1, minus_ref)):
        far_col = jnp.maximum(*key_col[way])
        far_row = jnp.maximum(*key_row[way])
        rank_row = count((far_col > far_row) | ((far_col == far_row) & (sub < lane)), 0)
        rank_col = count((far_row > far_col) | ((far_row == far_col) & (lane < sub)), 1)
        meta_ref[2, 4 + way : 5 + way, :] = rank_row
        chosen = rank_col == lane.astype(jnp.float32)
        for k in range(2):
            meta_ref[way, k : k + 1, :] = jnp.sum(jnp.where(chosen, q_col[k], 0.0), axis=0, keepdims=True)
            meta_ref[way, 2 + k : 3 + k, :] = jnp.sum(jnp.where(chosen, gcols[k], 0.0), axis=0, keepdims=True)
        meta_ref[way, 4:8, :] = jnp.zeros((4, rows), jnp.float32)
        order = jnp.where(sub.astype(jnp.float32) == rank_row, 1.0, 0.0).astype(jnp.bfloat16)
        for c in range(0, plan.width, 512):
            n = min(512, plan.width)
            out[:, c : c + n] = jnp.dot(
                order, normed[:, c : c + n], preferred_element_type=jnp.float32
            ).astype(jnp.bfloat16)
    meta_ref[2, 6:8, :] = jnp.zeros((2, rows), jnp.float32)


def sort_tokens(plan, tokens, gain_in, expert_ids, gate_weights):
    rows, width = plan.rows, plan.width
    return pl.pallas_call(
        functools.partial(sort_kernel, plan),
        out_shape=(
            jax.ShapeDtypeStruct((rows, width), jnp.bfloat16),
            jax.ShapeDtypeStruct((rows, width), jnp.bfloat16),
            jax.ShapeDtypeStruct((3, 8, rows), jnp.float32),
        ),
        in_specs=[VMEM] * 4,
        out_specs=(VMEM,) * 3,
        scratch_shapes=[pltpu.VMEM((rows, width), jnp.bfloat16)],
        compiler_params=pltpu.CompilerParams(vmem_limit_bytes=VMEM_LIMIT),
        name="sort_tokens",
    )(tokens, gain_in.reshape(1, width), expert_ids.T, gate_weights.T)


def hits(plan, meta, n, z, way, d, weighted):
    slots, cap = plan.slots, plan.cap
    slot = iota((slots, n), 0)
    base = z * slots
    total = jnp.zeros((slots, n), jnp.float32)
    for k in range(2):
        match = meta[k : k + 1, :n].astype(jnp.int32) - base == slot
        if d == plan.H:
            match = match & (slot < slots // 2 if way == 0 else slot >= slots // 2)
        total = total + jnp.where(match, meta[2 + k : 3 + k, :n] if weighted else 1.0, 0.0)
    return total


def last_hop(plan, p):
    return max(d for d in range(1, plan.H + 1) if plan.pieces[d] > p)


def experts_kernel(
    plan,
    plus_ref, minus_ref, meta_ref, wg_ref, wu_ref, wd_ref,
    out_ref,
    ring, back, metas, stage, arrived, rows_in, spread, doubled, wg, wu, wd, halves, final,
    zsend, zrecv, bsend, brecv, msend, mrecv, xsend, xrecv, ysend, yrecv,
    wsend, wrecv, wown, fsem,
):
    X, Z, H, cap, piece = plan.X, plan.Z, plan.H, plan.cap, plan.piece
    rows, width, slots = plan.rows, plan.width, plan.slots
    wide = min(512, width)
    z, x = plan.me()
    core = lax.axis_index("tp")
    other = 1 - core
    greet(plan, True)

    own = (plus_ref, minus_ref)
    outward = (plan.at(z + 1, x), plan.at(z - 1, x))
    homeward = (outward[1], outward[0])
    held = range(H // 2, H - 1)

    def late(d, p):
        return d in held and last_hop(plan, p) == d

    def places(d):
        if d == 0:
            return [(0, 0)]
        if d == H:
            return [(0, Z - 1), (1, Z - 1)]
        return [(0, 2 * d - 1), (1, 2 * d)]

    def spots(d):
        return sorted({j for _, j in places(d)})

    def passing(way, d, p):
        dst = ring.at[way, pl.ds(plan.offset[d] + p * piece, piece), :]
        if d == 1:
            src = own[way].at[pl.ds(p * piece, piece), :]
        else:
            src = ring.at[way, pl.ds(plan.offset[d - 1] + p * piece, piece), :]
        return remote(src, dst, zsend.at[way, d - 1, p], zrecv.at[way, d - 1, p], ep=outward[way])

    def passing_meta(way, d):
        src = meta_ref.at[way] if d == 1 else metas.at[way, d - 2]
        return remote(src, metas.at[way, d - 1], msend.at[way, d - 1], mrecv.at[way, d - 1], ep=outward[way])

    def closer(way, d, p):
        here = pl.ds(plan.offset[d] + p * piece, piece)
        return remote(
            ring.at[way, here, :], back.at[way, here, :],
            bsend.at[way, d - 1, p], brecv.at[way, d - 1, p], ep=homeward[way],
        )

    def column(r):
        return pl.ds(pl.multiple_of(lax.rem(x + r, X) * cap, cap), cap)

    def hand_over(j, r):
        src, dst = stage.at[j, column(r), :], arrived.at[j, column(0), :]
        return remote(src, dst, xsend.at[j, r], xrecv.at[j, r], ep=plan.at(z, x + r))

    def give_back(j, r):
        src, dst = arrived.at[j, column(r), :], rows_in.at[j, column(0), :]
        return remote(src, dst, ysend.at[j, r], yrecv.at[j, r], ep=plan.at(z, x + r))

    picked, computed = [], []

    def flush(waiting, copy):
        for j in waiting:
            for r in range(1, X):
                copy(j, r).start()
            if copy is hand_over:
                arrived[j, column(0), :] = stage[j, column(0), :]
            else:
                rows_in[j, column(0), :] = arrived[j, column(0), :]
        waiting.clear()

    def pick(way, d, j):
        n = rows if d == 0 else plan.prefix[d]
        meta = meta_ref[0] if d == 0 else metas[way, d - 1]
        source = plus_ref if d == 0 else ring.at[way, pl.ds(plan.offset[d], n), :]
        chosen = hits(plan, meta, n, z, way, d, False).astype(jnp.bfloat16)

        def columns(c, carry):
            here = pl.ds(pl.multiple_of(c * wide, wide), wide)
            found = jnp.dot(chosen, source[:, here], preferred_element_type=jnp.float32)
            found = found.astype(jnp.bfloat16)
            if d == H:
                lo = way * (slots // 2)
                stage[j, lo : lo + slots // 2, here] = found[lo : lo + slots // 2, :]
            else:
                stage[j, :, here] = found
            return carry

        lax.fori_loop(0, width // wide, columns, 0)

    def pick_all(d):
        for way, j in places(d):
            pick(way, d, j)
        picked.extend(spots(d))

    def land(d):
        for p in range(plan.pieces[d]):
            if late(d, p):
                for way in range(2):
                    passing(way, d, p).wait_recv()
        pick_all(d)

    def expert(j, carry):
        hidden = []
        for half in range(2):
            gated = jnp.dot(arrived[j], wg[half], preferred_element_type=jnp.float32)
            upward = jnp.dot(arrived[j], wu[half], preferred_element_type=jnp.float32)
            hidden.append((gated / (1.0 + jnp.exp(-gated)) * upward).astype(jnp.bfloat16))
        step = min(256, width)

        def down(c, carry):
            here = pl.ds(pl.multiple_of(c * step, step), step)
            total = jnp.zeros((slots, step), jnp.float32)
            for half in range(2):
                part = lax.dot_general(
                    hidden[half], wd[half, here, :], (((1,), (1,)), ((), ())),
                    preferred_element_type=jnp.float32,
                )
                total = total + part.astype(jnp.bfloat16).astype(jnp.float32)
            arrived[j, :, here] = total.astype(jnp.bfloat16)
            return carry

        lax.fori_loop(0, width // step, down, 0)
        return carry

    def compute(d):
        for j in spots(d):
            for r in range(1, X):
                hand_over(j, r).wait_recv()
        lax.fori_loop(spots(d)[0], spots(d)[-1] + 1, expert, 0)
        computed.extend(spots(d))

    def prepare(way, d, j):
        n = rows if d == 0 else plan.prefix[d]
        meta = meta_ref[2] if d == 0 else metas[way, d - 1]
        w = hits(plan, meta, n, z, way, d, True)
        high = w.astype(jnp.bfloat16).astype(jnp.float32)
        spread[way, :n, :] = jnp.concatenate([high, w - high], axis=0).T.astype(jnp.bfloat16)
        doubled[way, :slots, :] = rows_in[j]
        doubled[way, slots:, :] = rows_in[j]

    def wait_rows(d):
        for j in spots(d):
            for r in range(1, X):
                give_back(j, r).wait_recv()

    def combine(d):
        wait_rows(d)
        for way, j in places(d):
            prepare(way, d, j)
        if d < H:
            for way in range(2):
                for p in range(plan.pieces[d + 1]):
                    passing(way, d + 1, p).wait_send()

        def one(p, carry, joined):
            for way in range(2):
                if joined:
                    closer(way, d + 1, p).wait_recv()
                place = spread[way, pl.ds(pl.multiple_of(p * piece, piece), piece), :]
                mine = pl.ds(pl.multiple_of(plan.offset[d] + p * piece, piece), piece)
                for c in range(0, width, wide):
                    part = jnp.dot(
                        place, doubled[way, :, c : c + wide], preferred_element_type=jnp.float32
                    )
                    if joined:
                        there = pl.ds(pl.multiple_of(plan.offset[d + 1] + p * piece, piece), piece)
                        part = part + back[way, there, c : c + wide].astype(jnp.float32)
                    ring[way, mine, c : c + wide] = part.astype(jnp.bfloat16)
            for way in range(2):
                closer(way, d, p).start()
            return carry

        old, new = plan.pieces[d + 1], plan.pieces[d]
        if new > old:
            lax.fori_loop(old, new, functools.partial(one, joined=False), 0)
        if old:
            lax.fori_loop(0, old, functools.partial(one, joined=True), 0)

    for way in range(2):
        passing_meta(way, 1).start()
    for p in range(plan.pieces[1]):
        for way in range(2):
            passing(way, 1, p).start()
    weights = []
    for i, (src, dst) in enumerate(((wg_ref, wg), (wu_ref, wu), (wd_ref, wd))):
        weights.append(remote(src, dst.at[1], wsend.at[i], wrecv.at[i], tp=other))
        weights.append(pltpu.make_async_copy(src, dst.at[0], wown.at[i]))
    for copy in weights:
        copy.start()
    pick_all(0)
    done = []
    for d in range(1, H):
        for way in range(2):
            passing_meta(way, d).wait_recv()
            passing_meta(way, d + 1).start()
        for p in range(plan.pieces[d]):
            if not late(d, p):
                for way in range(2):
                    passing(way, d, p).wait_recv()
                    if p < plan.pieces[d + 1] and not late(d + 1, p):
                        passing(way, d + 1, p).start()
        flush(picked, hand_over)
        flush(computed, give_back)
        if d == H - 1:
            for e in reversed(held):
                for p in range(plan.pieces[e]):
                    if late(e, p):
                        for way in range(2):
                            passing(way, e, p).start()
        if d not in held:
            pick_all(d)
        if d == 1:
            for copy in weights:
                copy.wait()
        if 0 <= d - 2 < H // 2:
            compute(d - 2)
            done.append(d - 2)
    flush(picked, hand_over)
    flush(computed, give_back)

    rest = list(reversed(held))
    for way in range(2):
        passing_meta(way, H).wait_recv()
        for p in range(plan.pieces[H]):
            passing(way, H, p).wait_recv()
    pick_all(H)
    flush(picked, hand_over)
    for d in range(H // 2):
        if d not in done:
            compute(d)
    compute(H - 1)
    flush(computed, give_back)
    for d in rest[:1]:
        land(d)
        flush(picked, hand_over)
    compute(H)
    for d in rest[1:2]:
        land(d)
    flush(computed, give_back)
    flush(picked, hand_over)
    for d in rest[:1]:
        compute(d)
        flush(computed, give_back)
    combine(H)
    for d in rest[2:]:
        land(d)
        flush(picked, hand_over)
    combine(H - 1)
    for i, d in enumerate(rest):
        for e in rest[i + 1 : i + 2]:
            compute(e)
            flush(computed, give_back)
        combine(d)
    for d in range(H // 2 - 1, 0, -1):
        combine(d)

    wait_rows(0)
    prepare(0, 0, 0)
    order = []
    for way in range(2):
        slot = iota((rows, rows), 0).astype(jnp.float32)
        rank = meta_ref[2, 4 + way : 5 + way, :]
        order.append(jnp.where(slot == rank, 1.0, 0.0).T.astype(jnp.bfloat16))

        def arrive(p, carry, way=way):
            closer(way, 1, p).wait_recv()
            return carry

        lax.fori_loop(0, plan.pieces[1], arrive, 0)
    squares = jnp.zeros((rows, 1), jnp.float32)
    first = plan.offset[1]
    sums = []
    for c in range(0, width, wide):
        part = jnp.dot(spread[0], doubled[0, :, c : c + wide], preferred_element_type=jnp.float32)
        for way in range(2):
            part = part + jnp.dot(
                order[way], back[way, first : first + rows, c : c + wide],
                preferred_element_type=jnp.float32,
            )
        sums.append(part)
        squares = squares + jnp.sum(part * part, axis=1, keepdims=True)
    inverse = lax.rsqrt(squares / width + EPS)
    half_width = width // 2
    here = min(wide, half_width)
    for i, c in enumerate(range(0, width, wide)):
        scaled = (sums[i] * inverse).astype(jnp.bfloat16)
        for s in range(0, wide, here):
            halves[(c + s) // half_width, :, (c + s) % half_width : (c + s) % half_width + here] = (
                scaled[:, s : s + here]
            )
    mine = pl.ds(pl.multiple_of(core * rows, rows), rows)
    swap = remote(halves.at[other], final.at[mine, :], fsem.at[0], fsem.at[1], tp=other)
    swap.start()
    final[mine, :] = halves[core]

    for j in range(Z):
        for r in range(1, X):
            hand_over(j, r).wait_send()
            give_back(j, r).wait_send()
    for d in range(1, H + 1):
        for way in range(2):
            passing_meta(way, d).wait_send()

            def gone(p, carry, way=way, d=d):
                closer(way, d, p).wait_send()
                return carry

            lax.fori_loop(0, plan.pieces[d], gone, 0)
    for p in range(plan.pieces[1]):
        for way in range(2):
            passing(way, 1, p).wait_send()
    theirs = pl.ds(pl.multiple_of(other * rows, rows), rows)
    swap.wait_send()
    remote(halves.at[core], final.at[theirs, :], fsem.at[0], fsem.at[1], tp=other).wait_recv()
    out_ref[...] = final[...]


def run_experts(plan, plus, minus, meta, w_gate, w_up, w_down):
    X, Z, H, rows, width = plan.X, plan.Z, plan.H, plan.rows, plan.width
    dma = pltpu.SemaphoreType.DMA
    hops = (2, H, plan.most)
    bf16 = jnp.bfloat16
    return pl.pallas_call(
        functools.partial(experts_kernel, plan),
        out_shape=jax.ShapeDtypeStruct((2 * rows, width // 2), bf16),
        in_specs=[VMEM, VMEM, VMEM, ANY, ANY, ANY],
        out_specs=VMEM,
        scratch_shapes=[
            pltpu.VMEM((2, plan.total, width), bf16),
            pltpu.VMEM((2, plan.total, width), bf16),
            pltpu.VMEM((2, H, 8, rows), jnp.float32),
            pltpu.VMEM((Z, plan.slots, width), bf16),
            pltpu.VMEM((Z, plan.slots, width), bf16),
            pltpu.VMEM((Z, plan.slots, width), bf16),
            pltpu.VMEM((2, rows, 2 * plan.slots), bf16),
            pltpu.VMEM((2, 2 * plan.slots, width), bf16),
            pltpu.VMEM((2,) + w_gate.shape, bf16),
            pltpu.VMEM((2,) + w_up.shape, bf16),
            pltpu.VMEM((2,) + w_down.shape, bf16),
            pltpu.VMEM((2, rows, width // 2), bf16),
            pltpu.VMEM((2 * rows, width // 2), bf16),
            dma(hops), dma(hops), dma(hops), dma(hops), dma((2, H)), dma((2, H)),
            dma((Z, X)), dma((Z, X)), dma((Z, X)), dma((Z, X)),
            dma((3,)), dma((3,)), dma((3,)), dma((2,)),
        ],
        compiler_params=pltpu.CompilerParams(
            collective_id=0, has_side_effects=True, vmem_limit_bytes=VMEM_LIMIT
        ),
        name="run_experts",
    )(plus, minus, meta, w_gate, w_up, w_down)


def per_device(columns, tokens, gain_in, expert_ids, gate_weights, w_gate, w_up, w_down, gain_out):
    own_rows, width = tokens.shape
    members = lax.axis_size("ep")
    capacity = 2 * own_rows * expert_ids.shape[1] // members
    plan = Plan(own_rows, width, members, capacity, columns)
    plus, minus, meta = sort_tokens(plan, tokens, gain_in, expert_ids, gate_weights)
    scaled = run_experts(plan, plus, minus, meta, w_gate[0], w_up[0], w_down[0])
    return (scaled.astype(jnp.float32) * gain_out).astype(jnp.bfloat16)


def solution(mesh, columns=COLUMNS):
    placed = (
        P(("grp", "ep", "tp"), None),
        P(),
        P(("grp", "ep"), None),
        P(("grp", "ep"), None),
        P("ep", None, "tp"),
        P("ep", None, "tp"),
        P("ep", None, "tp"),
        P("tp"),
    )
    return jax.shard_map(
        functools.partial(per_device, columns),
        mesh=mesh, in_specs=placed, out_specs=P(("grp", "ep"), "tp"), check_vma=False,
    )
```

```python
import functools

import jax
import jax.numpy as jnp
from jax import lax
from jax.experimental import pallas as pl
from jax.experimental.pallas import tpu as pltpu
from jax.sharding import PartitionSpec as P

EPS = 1e-06
COLUMNS = 4
MESH = pl.DeviceIdType.MESH
VMEM = pl.BlockSpec(memory_space=pltpu.VMEM)
ANY = pl.BlockSpec(memory_space=pl.ANY)
VMEM_LIMIT = 60 * 1024 * 1024


class Plan:
    def __init__(self, rows, width, members, capacity, columns):
        self.rows, self.width, self.members, self.cap, self.X = rows, width, members, capacity, columns
        self.Z = members // columns
        self.H = self.Z // 2
        self.slots = columns * capacity
        self.piece = self.slots // 2
        self.prefix = [0] + [
            min(rows, (self.H - d) * self.slots + self.slots // 2) for d in range(1, self.H + 1)
        ] + [0]
        self.pieces = [n // self.piece for n in self.prefix]
        self.offset = [sum(self.prefix[:d]) for d in range(self.H + 2)]
        self.total = sum(self.prefix)
        self.most = max(self.pieces)

    def me(self):
        ep = lax.axis_index("ep")
        return ep // self.X, ep % self.X

    def at(self, z, x):
        return lax.rem(z + 2 * self.Z, self.Z) * self.X + lax.rem(x + 2 * self.X, self.X)


def remote(src, dst, send, recv, **where):
    return pltpu.make_async_remote_copy(
        src_ref=src, dst_ref=dst, send_sem=send, recv_sem=recv, device_id=where, device_id_type=MESH
    )


def greet(plan):
    z, x = plan.me()
    peers = [{"ep": plan.at(z + 1, x)}, {"ep": plan.at(z - 1, x)}]
    peers += [{"ep": plan.at(z, x + r)} for r in range(1, plan.X)]
    peers.append({"tp": 1 - lax.axis_index("tp")})
    barrier = pltpu.get_barrier_semaphore()
    for peer in peers:
        pl.semaphore_signal(barrier, inc=1, device_id=peer, device_id_type=MESH)
    return barrier, len(peers)


def iota(shape, dim):
    return lax.broadcasted_iota(jnp.int32, shape, dim)


def sort_tokens(plan, x_ref, gain_ref, ids_ref, gates_ref, plus_ref, minus_ref, meta_ref, normed):
    rows, X, Z, H = plan.rows, plan.X, plan.Z, plan.H
    z, _ = plan.me()
    step = 32

    def norm_step(i, carry):
        here = pl.ds(pl.multiple_of(i * step, step), step)
        x = x_ref[here, :].astype(jnp.float32)
        scale = lax.rsqrt(jnp.mean(x * x, axis=1, keepdims=True) + EPS)
        normed[here, :] = (x * scale * gain_ref[...]).astype(jnp.bfloat16)
        return carry

    lax.fori_loop(0, rows // step, norm_step, 0)

    own = pl.ds(pl.multiple_of(lax.axis_index("tp") * rows, rows), rows)
    square = (rows, rows)
    sub, lane = iota(square, 0), iota(square, 1)
    eye = sub == lane

    def as_column(row):
        return jnp.sum(jnp.where(eye, row, 0.0), axis=1, keepdims=True)

    def count(mask, axis):
        return jnp.sum(jnp.where(mask, 1.0, 0.0), axis=axis, keepdims=True)

    rws = [ids_ref[k : k + 1, own].astype(jnp.float32) for k in range(2)]
    cols = [as_column(r) for r in rws]
    grws = [gates_ref[k : k + 1, own] for k in range(2)]
    gcols = [as_column(g) for g in grws]
    q_col, q_row, key_col, key_row = [], [], [[], []], [[], []]
    for k in range(2):
        slot_row = count((sub < lane) & (cols[0] == rws[k]), 0) + count((sub < lane) & (cols[1] == rws[k]), 0)
        slot_col = count((lane < sub) & (rws[0] == cols[k]), 1) + count((lane < sub) & (rws[1] == cols[k]), 1)
        q_row.append(rws[k] * plan.cap + slot_row)
        q_col.append(cols[k] * plan.cap + slot_col)
        for expert, keys in ((rws[k], key_row), (cols[k], key_col)):
            e = expert.astype(jnp.int32)
            ahead = e // X - z
            ahead = jnp.where(ahead < 0, ahead + Z, ahead)
            first = e % X < X // 2
            up = jnp.where((ahead < H) | ((ahead == H) & first), ahead, 0)
            down = jnp.where((ahead > H) | ((ahead == H) & ~first), Z - ahead, 0)
            keys[0].append(up.astype(jnp.float32))
            keys[1].append(down.astype(jnp.float32))
    for k in range(2):
        meta_ref[2, k : k + 1, :] = q_row[k]
        meta_ref[2, 2 + k : 3 + k, :] = grws[k]
    for way, out in ((0, plus_ref), (1, minus_ref)):
        far_col = jnp.maximum(*key_col[way])
        far_row = jnp.maximum(*key_row[way])
        rank_row = count((far_col > far_row) | ((far_col == far_row) & (sub < lane)), 0)
        rank_col = count((far_row > far_col) | ((far_row == far_col) & (lane < sub)), 1)
        meta_ref[2, 4 + way : 5 + way, :] = rank_row
        chosen = rank_col == lane.astype(jnp.float32)
        for k in range(2):
            meta_ref[way, k : k + 1, :] = jnp.sum(jnp.where(chosen, q_col[k], 0.0), axis=0, keepdims=True)
            meta_ref[way, 2 + k : 3 + k, :] = jnp.sum(jnp.where(chosen, gcols[k], 0.0), axis=0, keepdims=True)
        meta_ref[way, 4:8, :] = jnp.zeros((4, rows), jnp.float32)
        order = jnp.where(sub.astype(jnp.float32) == rank_row, 1.0, 0.0).astype(jnp.bfloat16)
        for c in range(0, plan.width, 512):
            n = min(512, plan.width)
            out[:, c : c + n] = jnp.dot(
                order, normed[:, c : c + n], preferred_element_type=jnp.float32
            ).astype(jnp.bfloat16)
    meta_ref[2, 6:8, :] = jnp.zeros((2, rows), jnp.float32)


def hits(plan, meta, n, z, way, d, weighted):
    slots, cap = plan.slots, plan.cap
    slot = iota((slots, n), 0)
    base = z * slots
    total = jnp.zeros((slots, n), jnp.float32)
    for k in range(2):
        match = meta[k : k + 1, :n].astype(jnp.int32) - base == slot
        if d == plan.H:
            match = match & (slot < slots // 2 if way == 0 else slot >= slots // 2)
        total = total + jnp.where(match, meta[2 + k : 3 + k, :n] if weighted else 1.0, 0.0)
    return total


def schedule(plan):
    if plan.pieces != [0, 8, 8, 8, 8, 7, 5, 3, 1, 0]:
        raise ValueError("no schedule")

    def go(*pieces):
        return [("go", d, p) for d, p in pieces]

    def expert(d):
        return [("expert", d, 0), ("expert", d, 1)]

    def first(d):
        return go((d, 0), (d, 1), (d, 2))

    return (
        first(1) + [("pick", 0)] + first(2) + first(3) + first(4) + [("expert", 0, 0)]
        + first(5) + first(6) + first(7)
        + go((1, 3), (8, 0), (1, 4), (1, 5)) + [("pick", 7)]
        + go((2, 3), (2, 4), (1, 6)) + [("pick", 8)]
        + go((3, 3), (3, 4), (2, 5)) + [("expert", 7, 0)]
        + go((4, 3), (4, 4), (2, 6)) + [("expert", 7, 1)]
        + go((5, 3), (5, 4), (3, 5)) + [("expert", 8, 0)]
        + go((6, 3), (6, 4), (3, 6), (1, 7), (4, 5), (4, 6)) + [("pick", 6)]
        + go((2, 7), (5, 5), (5, 6)) + expert(6)
        + go((3, 7)) + [("sum", 8), ("pick", 5), ("sum", 7)]
        + go((4, 7)) + expert(5) + [("sum", 6), ("pick", 4), ("pick", 3), ("sum", 5)]
        + expert(4) + expert(3) + [("sum", 4), ("pick", 2), ("pick", 1)]
        + expert(2) + [("sum", 3)] + expert(1) + [("sum", 2), ("sum", 1)]
    )


def experts_kernel(
    plan,
    x_ref, gain_ref, ids_ref, gates_ref, wg_ref, wu_ref, wd_ref,
    out_ref,
    normed, plus_ref, minus_ref, meta_ref, ring, back, metas, stage, arrived, rows_in, spread, doubled, wg, wu, wd, halves, final,
    zsend, zrecv, bsend, brecv, msend, mrecv, xsend, xrecv, ysend, yrecv,
    wsend, wrecv, wown, fsem,
):
    X, Z, H, cap, piece = plan.X, plan.Z, plan.H, plan.cap, plan.piece
    rows, width, slots = plan.rows, plan.width, plan.slots
    wide = min(512, width)
    z, x = plan.me()
    core = lax.axis_index("tp")
    other = 1 - core
    barrier, peers = greet(plan)
    sort_tokens(plan, x_ref, gain_ref, ids_ref, gates_ref, plus_ref, minus_ref, meta_ref, normed)
    pl.semaphore_wait(barrier, peers)

    own = (plus_ref, minus_ref)
    outward = (plan.at(z + 1, x), plan.at(z - 1, x))
    homeward = (outward[1], outward[0])
    def places(d):
        if d == 0:
            return [(0, 0)]
        if d == H:
            return [(0, Z - 1), (1, Z - 1)]
        return [(0, 2 * d - 1), (1, 2 * d)]

    def spots(d):
        return sorted({j for _, j in places(d)})

    def passing(way, d, p):
        dst = ring.at[way, pl.ds(plan.offset[d] + p * piece, piece), :]
        if d == 1:
            src = own[way].at[pl.ds(p * piece, piece), :]
        else:
            src = ring.at[way, pl.ds(plan.offset[d - 1] + p * piece, piece), :]
        return remote(src, dst, zsend.at[way, d - 1, p], zrecv.at[way, d - 1, p], ep=outward[way])

    def passing_meta(way, d):
        src = meta_ref.at[way] if d == 1 else metas.at[way, d - 2]
        return remote(src, metas.at[way, d - 1], msend.at[way, d - 1], mrecv.at[way, d - 1], ep=outward[way])

    def closer(way, d, p):
        here = pl.ds(plan.offset[d] + p * piece, piece)
        return remote(
            ring.at[way, here, :], back.at[way, here, :],
            bsend.at[way, d - 1, p], brecv.at[way, d - 1, p], ep=homeward[way],
        )

    def column(r):
        return pl.ds(pl.multiple_of(lax.rem(x + r, X) * cap, cap), cap)

    def hand_over(j, r):
        src, dst = stage.at[j, column(r), :], arrived.at[j, column(0), :]
        return remote(src, dst, xsend.at[j, r], xrecv.at[j, r], ep=plan.at(z, x + r))

    def give_back(j, r):
        src, dst = arrived.at[j, column(r), :], rows_in.at[j, column(0), :]
        return remote(src, dst, ysend.at[j, r], yrecv.at[j, r], ep=plan.at(z, x + r))

    def exchange(j, copy):
        for r in range(1, X):
            copy(j, r).start()
        if copy is hand_over:
            arrived[j, column(0), :] = stage[j, column(0), :]
        else:
            rows_in[j, column(0), :] = arrived[j, column(0), :]

    def pick(way, d, j):
        n = rows if d == 0 else plan.prefix[d]
        meta = meta_ref[0] if d == 0 else metas[way, d - 1]
        source = plus_ref if d == 0 else ring.at[way, pl.ds(plan.offset[d], n), :]
        chosen = hits(plan, meta, n, z, way, d, False).astype(jnp.bfloat16)

        def columns(c, carry):
            here = pl.ds(pl.multiple_of(c * wide, wide), wide)
            found = jnp.dot(chosen, source[:, here], preferred_element_type=jnp.float32)
            found = found.astype(jnp.bfloat16)
            if d == H:
                lo = way * (slots // 2)
                stage[j, lo : lo + slots // 2, here] = found[lo : lo + slots // 2, :]
            else:
                stage[j, :, here] = found
            return carry

        lax.fori_loop(0, width // wide, columns, 0)

    landed = set()

    def await_piece(d, p):
        if (d, p) not in landed:
            for way in range(2):
                passing(way, d, p).wait_recv()
            landed.add((d, p))

    def pass_on(d, p):
        for way in range(2):
            if p == 0 and d > 1:
                passing_meta(way, d - 1).wait_recv()
            if p == 0:
                passing_meta(way, d).start()
        if d > 1:
            await_piece(d - 1, p)
        for way in range(2):
            passing(way, d, p).start()

    def pick_plane(d):
        if d == H:
            for way in range(2):
                passing_meta(way, d).wait_recv()
        for p in range(plan.pieces[d]):
            await_piece(d, p)
        for way, j in places(d):
            pick(way, d, j)
        for j in spots(d):
            exchange(j, hand_over)

    def expert(j):
        hidden = []
        for half in range(2):
            gated = jnp.dot(arrived[j], wg[half], preferred_element_type=jnp.float32)
            upward = jnp.dot(arrived[j], wu[half], preferred_element_type=jnp.float32)
            hidden.append((gated / (1.0 + jnp.exp(-gated)) * upward).astype(jnp.bfloat16))
        step = min(256, width)

        def down(c, carry):
            here = pl.ds(pl.multiple_of(c * step, step), step)
            total = jnp.zeros((slots, step), jnp.float32)
            for half in range(2):
                part = lax.dot_general(
                    hidden[half], wd[half, here, :], (((1,), (1,)), ((), ())),
                    preferred_element_type=jnp.float32,
                )
                total = total + part.astype(jnp.bfloat16).astype(jnp.float32)
            arrived[j, :, here] = total.astype(jnp.bfloat16)
            return carry

        lax.fori_loop(0, width // step, down, 0)

    def compute(d, n):
        j = spots(d)[n]
        for r in range(1, X):
            hand_over(j, r).wait_recv()
        expert(j)
        exchange(j, give_back)

    def prepare(way, d, j):
        n = rows if d == 0 else plan.prefix[d]
        meta = meta_ref[2] if d == 0 else metas[way, d - 1]
        w = hits(plan, meta, n, z, way, d, True)
        high = w.astype(jnp.bfloat16).astype(jnp.float32)
        spread[way, :n, :] = jnp.concatenate([high, w - high], axis=0).T.astype(jnp.bfloat16)
        doubled[way, :slots, :] = rows_in[j]
        doubled[way, slots:, :] = rows_in[j]

    def wait_rows(d):
        for j in spots(d):
            for r in range(1, X):
                give_back(j, r).wait_recv()

    def combine(d):
        wait_rows(d)
        for way, j in places(d):
            prepare(way, d, j)
        if d < H:
            for way in range(2):
                for p in range(plan.pieces[d + 1]):
                    passing(way, d + 1, p).wait_send()

        def one(p, carry, joined):
            for way in range(2):
                if joined:
                    closer(way, d + 1, p).wait_recv()
                place = spread[way, pl.ds(pl.multiple_of(p * piece, piece), piece), :]
                mine = pl.ds(pl.multiple_of(plan.offset[d] + p * piece, piece), piece)
                for c in range(0, width, wide):
                    part = jnp.dot(
                        place, doubled[way, :, c : c + wide], preferred_element_type=jnp.float32
                    )
                    if joined:
                        there = pl.ds(pl.multiple_of(plan.offset[d + 1] + p * piece, piece), piece)
                        part = part + back[way, there, c : c + wide].astype(jnp.float32)
                    ring[way, mine, c : c + wide] = part.astype(jnp.bfloat16)
            for way in range(2):
                closer(way, d, p).start()
            return carry

        old, new = plan.pieces[d + 1], plan.pieces[d]
        if new > old:
            lax.fori_loop(old, new, functools.partial(one, joined=False), 0)
        if old:
            lax.fori_loop(0, old, functools.partial(one, joined=True), 0)

    weights = []
    for i, (src, dst) in enumerate(((wg_ref, wg), (wu_ref, wu), (wd_ref, wd))):
        weights.append(remote(src, dst.at[1], wsend.at[i], wrecv.at[i], tp=other))
        weights.append(pltpu.make_async_copy(src, dst.at[0], wown.at[i]))
    for i, (kind, d, *which) in enumerate(schedule(plan)):
        if kind == "go":
            pass_on(d, *which)
        elif kind == "pick":
            pick_plane(d)
        elif kind == "expert":
            if d == 0:
                for copy in weights:
                    copy.wait()
            compute(d, *which)
        else:
            combine(d)
        if i == 2:
            for copy in weights:
                copy.start()

    wait_rows(0)
    prepare(0, 0, 0)
    order = []
    for way in range(2):
        slot = iota((rows, rows), 0).astype(jnp.float32)
        rank = meta_ref[2, 4 + way : 5 + way, :]
        order.append(jnp.where(slot == rank, 1.0, 0.0).T.astype(jnp.bfloat16))

        def arrive(p, carry, way=way):
            closer(way, 1, p).wait_recv()
            return carry

        lax.fori_loop(0, plan.pieces[1], arrive, 0)
    squares = jnp.zeros((rows, 1), jnp.float32)
    first = plan.offset[1]
    sums = []
    for c in range(0, width, wide):
        part = jnp.dot(spread[0], doubled[0, :, c : c + wide], preferred_element_type=jnp.float32)
        for way in range(2):
            part = part + jnp.dot(
                order[way], back[way, first : first + rows, c : c + wide],
                preferred_element_type=jnp.float32,
            )
        sums.append(part)
        squares = squares + jnp.sum(part * part, axis=1, keepdims=True)
    inverse = lax.rsqrt(squares / width + EPS)
    half_width = width // 2
    here = min(wide, half_width)
    for i, c in enumerate(range(0, width, wide)):
        scaled = (sums[i] * inverse).astype(jnp.bfloat16)
        for s in range(0, wide, here):
            halves[(c + s) // half_width, :, (c + s) % half_width : (c + s) % half_width + here] = (
                scaled[:, s : s + here]
            )
    mine = pl.ds(pl.multiple_of(core * rows, rows), rows)
    swap = remote(halves.at[other], final.at[mine, :], fsem.at[0], fsem.at[1], tp=other)
    swap.start()
    final[mine, :] = halves[core]

    for j in range(Z):
        for r in range(1, X):
            hand_over(j, r).wait_send()
            give_back(j, r).wait_send()
    for d in range(1, H + 1):
        for way in range(2):
            passing_meta(way, d).wait_send()

            def gone(p, carry, way=way, d=d):
                closer(way, d, p).wait_send()
                return carry

            lax.fori_loop(0, plan.pieces[d], gone, 0)
    for p in range(plan.pieces[1]):
        for way in range(2):
            passing(way, 1, p).wait_send()
    theirs = pl.ds(pl.multiple_of(other * rows, rows), rows)
    swap.wait_send()
    remote(halves.at[core], final.at[theirs, :], fsem.at[0], fsem.at[1], tp=other).wait_recv()
    out_ref[...] = final[...]


def run_experts(plan, tokens, gain_in, expert_ids, gate_weights, w_gate, w_up, w_down):
    X, Z, H, rows, width = plan.X, plan.Z, plan.H, plan.rows, plan.width
    dma = pltpu.SemaphoreType.DMA
    hops = (2, H, plan.most)
    bf16 = jnp.bfloat16
    return pl.pallas_call(
        functools.partial(experts_kernel, plan),
        out_shape=jax.ShapeDtypeStruct((2 * rows, width // 2), bf16),
        in_specs=[VMEM, VMEM, VMEM, VMEM, ANY, ANY, ANY],
        out_specs=VMEM,
        scratch_shapes=[
            pltpu.VMEM((rows, width), bf16),
            pltpu.VMEM((rows, width), bf16),
            pltpu.VMEM((rows, width), bf16),
            pltpu.VMEM((3, 8, rows), jnp.float32),
            pltpu.VMEM((2, plan.total, width), bf16),
            pltpu.VMEM((2, plan.total, width), bf16),
            pltpu.VMEM((2, H, 8, rows), jnp.float32),
            pltpu.VMEM((Z, plan.slots, width), bf16),
            pltpu.VMEM((Z, plan.slots, width), bf16),
            pltpu.VMEM((Z, plan.slots, width), bf16),
            pltpu.VMEM((2, rows, 2 * plan.slots), bf16),
            pltpu.VMEM((2, 2 * plan.slots, width), bf16),
            pltpu.VMEM((2,) + w_gate.shape, bf16),
            pltpu.VMEM((2,) + w_up.shape, bf16),
            pltpu.VMEM((2,) + w_down.shape, bf16),
            pltpu.VMEM((2, rows, width // 2), bf16),
            pltpu.VMEM((2 * rows, width // 2), bf16),
            dma(hops), dma(hops), dma(hops), dma(hops), dma((2, H)), dma((2, H)),
            dma((Z, X)), dma((Z, X)), dma((Z, X)), dma((Z, X)),
            dma((3,)), dma((3,)), dma((3,)), dma((2,)),
        ],
        compiler_params=pltpu.CompilerParams(
            collective_id=0, has_side_effects=True, vmem_limit_bytes=VMEM_LIMIT
        ),
        name="run_experts",
    )(tokens, gain_in.reshape(1, width), expert_ids.T, gate_weights.T, w_gate, w_up, w_down)


def per_device(columns, tokens, gain_in, expert_ids, gate_weights, w_gate, w_up, w_down, gain_out):
    own_rows, width = tokens.shape
    members = lax.axis_size("ep")
    capacity = 2 * own_rows * expert_ids.shape[1] // members
    plan = Plan(own_rows, width, members, capacity, columns)
    scaled = run_experts(
        plan, tokens, gain_in, expert_ids, gate_weights, w_gate[0], w_up[0], w_down[0]
    )
    return (scaled.astype(jnp.float32) * gain_out).astype(jnp.bfloat16)


def solution(mesh, columns=COLUMNS):
    placed = (
        P(("grp", "ep", "tp"), None),
        P(),
        P(("grp", "ep"), None),
        P(("grp", "ep"), None),
        P("ep", None, "tp"),
        P("ep", None, "tp"),
        P("ep", None, "tp"),
        P("tp"),
    )
    return jax.shard_map(
        functools.partial(per_device, columns),
        mesh=mesh, in_specs=placed, out_specs=P(("grp", "ep"), "tp"), check_vma=False,
    )
```

```python
import functools

import jax
import jax.numpy as jnp
from jax import lax
from jax.experimental import pallas as pl
from jax.experimental.pallas import tpu as pltpu
from jax.sharding import PartitionSpec as P

EPS = 1e-06
COLUMNS = 4
MESH = pl.DeviceIdType.MESH
VMEM = pl.BlockSpec(memory_space=pltpu.VMEM)
ANY = pl.BlockSpec(memory_space=pl.ANY)
VMEM_LIMIT = 60 * 1024 * 1024


class Plan:
    def __init__(self, rows, width, members, capacity, columns):
        self.rows, self.width, self.members, self.cap, self.X = rows, width, members, capacity, columns
        self.Z = members // columns
        self.H = self.Z // 2
        self.slots = columns * capacity
        self.piece = self.slots // 2
        self.prefix = [0] + [
            min(rows, (self.H - d) * self.slots + self.slots // 2) for d in range(1, self.H + 1)
        ] + [0]
        self.pieces = [n // self.piece for n in self.prefix]
        self.offset = [sum(self.prefix[:d]) for d in range(self.H + 2)]
        self.total = sum(self.prefix)
        self.most = max(self.pieces)

    def number(self, d, p):
        return self.offset[d] // self.piece + p

    def me(self):
        ep = lax.axis_index("ep")
        return ep // self.X, ep % self.X

    def at(self, z, x):
        return lax.rem(z + 2 * self.Z, self.Z) * self.X + lax.rem(x + 2 * self.X, self.X)


def remote(src, dst, send, recv, **where):
    return pltpu.make_async_remote_copy(
        src_ref=src, dst_ref=dst, send_sem=send, recv_sem=recv, device_id=where, device_id_type=MESH
    )


def greet(plan):
    z, x = plan.me()
    peers = [{"ep": plan.at(z + 1, x)}, {"ep": plan.at(z - 1, x)}]
    peers += [{"ep": plan.at(z, x + r)} for r in range(1, plan.X)]
    peers.append({"tp": 1 - lax.axis_index("tp")})
    barrier = pltpu.get_barrier_semaphore()
    for peer in peers:
        pl.semaphore_signal(barrier, inc=1, device_id=peer, device_id_type=MESH)
    return barrier, len(peers)


def iota(shape, dim):
    return lax.broadcasted_iota(jnp.int32, shape, dim)


def sort_tokens(plan, x_ref, gain_ref, ids_ref, gates_ref, plus_ref, minus_ref, meta_ref, normed):
    rows, X, Z, H = plan.rows, plan.X, plan.Z, plan.H
    z, _ = plan.me()
    step = 32

    def norm_step(i, carry):
        here = pl.ds(pl.multiple_of(i * step, step), step)
        x = x_ref[here, :].astype(jnp.float32)
        scale = lax.rsqrt(jnp.mean(x * x, axis=1, keepdims=True) + EPS)
        normed[here, :] = (x * scale * gain_ref[...]).astype(jnp.bfloat16)
        return carry

    lax.fori_loop(0, rows // step, norm_step, 0)

    own = pl.ds(pl.multiple_of(lax.axis_index("tp") * rows, rows), rows)
    square = (rows, rows)
    sub, lane = iota(square, 0), iota(square, 1)
    eye = sub == lane

    def as_column(row):
        return jnp.sum(jnp.where(eye, row, 0.0), axis=1, keepdims=True)

    def count(mask, axis):
        return jnp.sum(jnp.where(mask, 1.0, 0.0), axis=axis, keepdims=True)

    rws = [ids_ref[k : k + 1, own].astype(jnp.float32) for k in range(2)]
    cols = [as_column(r) for r in rws]
    grws = [gates_ref[k : k + 1, own] for k in range(2)]
    gcols = [as_column(g) for g in grws]
    q_col, q_row, key_col, key_row = [], [], [[], []], [[], []]
    for k in range(2):
        slot_row = count((sub < lane) & (cols[0] == rws[k]), 0) + count((sub < lane) & (cols[1] == rws[k]), 0)
        slot_col = count((lane < sub) & (rws[0] == cols[k]), 1) + count((lane < sub) & (rws[1] == cols[k]), 1)
        q_row.append(rws[k] * plan.cap + slot_row)
        q_col.append(cols[k] * plan.cap + slot_col)
        for expert, keys in ((rws[k], key_row), (cols[k], key_col)):
            e = expert.astype(jnp.int32)
            ahead = e // X - z
            ahead = jnp.where(ahead < 0, ahead + Z, ahead)
            first = e % X < X // 2
            up = jnp.where((ahead < H) | ((ahead == H) & first), ahead, 0)
            down = jnp.where((ahead > H) | ((ahead == H) & ~first), Z - ahead, 0)
            keys[0].append(up.astype(jnp.float32))
            keys[1].append(down.astype(jnp.float32))
    for k in range(2):
        meta_ref[2, k : k + 1, :] = q_row[k]
        meta_ref[2, 2 + k : 3 + k, :] = grws[k]
    for way, out in ((0, plus_ref), (1, minus_ref)):
        far_col = jnp.maximum(*key_col[way])
        far_row = jnp.maximum(*key_row[way])
        rank_row = count((far_col > far_row) | ((far_col == far_row) & (sub < lane)), 0)
        rank_col = count((far_row > far_col) | ((far_row == far_col) & (lane < sub)), 1)
        meta_ref[2, 4 + way : 5 + way, :] = rank_row
        chosen = rank_col == lane.astype(jnp.float32)
        for k in range(2):
            meta_ref[way, k : k + 1, :] = jnp.sum(jnp.where(chosen, q_col[k], 0.0), axis=0, keepdims=True)
            meta_ref[way, 2 + k : 3 + k, :] = jnp.sum(jnp.where(chosen, gcols[k], 0.0), axis=0, keepdims=True)
        meta_ref[way, 4:8, :] = jnp.zeros((4, rows), jnp.float32)
        order = jnp.where(sub.astype(jnp.float32) == rank_row, 1.0, 0.0).astype(jnp.bfloat16)
        for c in range(0, plan.width, 512):
            n = min(512, plan.width)
            out[:, c : c + n] = jnp.dot(
                order, normed[:, c : c + n], preferred_element_type=jnp.float32
            ).astype(jnp.bfloat16)
    meta_ref[2, 6:8, :] = jnp.zeros((2, rows), jnp.float32)


def hits(plan, meta, n, z, way, d, weighted):
    slots, cap = plan.slots, plan.cap
    slot = iota((slots, n), 0)
    base = z * slots
    total = jnp.zeros((slots, n), jnp.float32)
    for k in range(2):
        match = meta[k : k + 1, :n].astype(jnp.int32) - base == slot
        if d == plan.H:
            match = match & (slot < slots // 2 if way == 0 else slot >= slots // 2)
        total = total + jnp.where(match, meta[2 + k : 3 + k, :n] if weighted else 1.0, 0.0)
    return total


def schedule(plan):
    if plan.pieces != [0, 8, 8, 8, 8, 7, 5, 3, 1, 0]:
        raise ValueError("no schedule")

    def go(*pieces):
        return [("go", d, p) for d, p in pieces]

    def expert(d):
        return [("expert", d, 0), ("expert", d, 1)]

    def first(d):
        return go((d, 0), (d, 1), (d, 2))

    return (
        first(1) + [("pick", 0)] + first(2) + first(3) + first(4) + [("expert", 0, 0)]
        + first(5) + first(6) + first(7)
        + go((1, 3), (8, 0), (1, 4), (1, 5)) + [("pick", 7)]
        + go((2, 3), (2, 4), (1, 6)) + [("pick", 8)]
        + go((3, 3), (3, 4), (2, 5)) + [("expert", 7, 0)]
        + go((4, 3), (4, 4), (2, 6)) + [("expert", 7, 1)]
        + go((5, 3), (5, 4), (3, 5)) + [("expert", 8, 0)]
        + go((6, 3), (6, 4), (3, 6), (1, 7), (4, 5), (4, 6)) + [("pick", 6)]
        + go((2, 7), (5, 5), (5, 6)) + expert(6)
        + go((3, 7)) + [("sum", 8), ("pick", 5), ("sum", 7)]
        + go((4, 7)) + expert(5) + [("sum", 6), ("pick", 4), ("pick", 3), ("sum", 5)]
        + expert(4) + expert(3) + [("sum", 4), ("pick", 2), ("pick", 1)]
        + expert(2) + [("sum", 3)] + expert(1) + [("sum", 2), ("sum", 1)]
    )


def experts_kernel(
    plan,
    x_ref, gain_ref, ids_ref, gates_ref, wg_ref, wu_ref, wd_ref, gain_out_ref,
    out_ref,
    normed, plus_ref, minus_ref, meta_ref, ring, back, metas, stage, arrived, rows_in, spread, doubled,
    wg, wu, wd, halves, final,
    zsend, zrecv, bsend, brecv, msend, mrecv, xsend, xrecv, ysend, yrecv,
    wsend, wrecv, wown, fsem,
):
    X, Z, H, cap, piece = plan.X, plan.Z, plan.H, plan.cap, plan.piece
    rows, width, slots = plan.rows, plan.width, plan.slots
    wide = min(512, width)
    z, x = plan.me()
    core = lax.axis_index("tp")
    other = 1 - core
    barrier, peers = greet(plan)
    sort_tokens(plan, x_ref, gain_ref, ids_ref, gates_ref, plus_ref, minus_ref, meta_ref, normed)
    pl.semaphore_wait(barrier, peers)

    own = (plus_ref, minus_ref)
    outward = (plan.at(z + 1, x), plan.at(z - 1, x))
    homeward = (outward[1], outward[0])
    def places(d):
        if d == 0:
            return [(0, 0)]
        if d == H:
            return [(0, Z - 1), (1, Z - 1)]
        return [(0, 2 * d - 1), (1, 2 * d)]

    def spots(d):
        return sorted({j for _, j in places(d)})

    def passing(way, d, p):
        dst = ring.at[way, pl.ds(plan.offset[d] + p * piece, piece), :]
        if d == 1:
            src = own[way].at[pl.ds(p * piece, piece), :]
        else:
            src = ring.at[way, pl.ds(plan.offset[d - 1] + p * piece, piece), :]
        return remote(src, dst, zsend.at[way, d - 1], zrecv.at[way, plan.number(d, p)], ep=outward[way])

    def passing_meta(way, d):
        src = meta_ref.at[way] if d == 1 else metas.at[way, d - 2]
        return remote(src, metas.at[way, d - 1], msend.at[0], mrecv.at[way, d - 1], ep=outward[way])

    def closer(way, d, p):
        here = pl.ds(plan.offset[d] + p * piece, piece)
        return remote(
            ring.at[way, here, :], back.at[way, here, :],
            bsend.at[way], brecv.at[way, plan.number(d, p)], ep=homeward[way],
        )

    def column(r):
        return pl.ds(pl.multiple_of(lax.rem(x + r, X) * cap, cap), cap)

    def hand_over(j, r):
        src, dst = stage.at[j, column(r), :], arrived.at[j, column(0), :]
        return remote(src, dst, xsend.at[0], xrecv.at[j], ep=plan.at(z, x + r))

    def give_back(j, r):
        src, dst = arrived.at[j, column(r), :], rows_in.at[j, column(0), :]
        return remote(src, dst, ysend.at[0], yrecv.at[j], ep=plan.at(z, x + r))

    def all_columns(j, ref, send, recv):
        part = ref.at[j, pl.ds(0, plan.slots - cap), :]
        return remote(part, part, send, recv, ep=plan.at(z, x + 1))

    def exchange(j, copy):
        for r in range(1, X):
            copy(j, r).start()
        if copy is hand_over:
            arrived[j, column(0), :] = stage[j, column(0), :]
        else:
            rows_in[j, column(0), :] = arrived[j, column(0), :]

    def pick(way, d, j):
        n = rows if d == 0 else plan.prefix[d]
        meta = meta_ref[0] if d == 0 else metas[way, d - 1]
        source = plus_ref if d == 0 else ring.at[way, pl.ds(plan.offset[d], n), :]
        chosen = hits(plan, meta, n, z, way, d, False).astype(jnp.bfloat16)

        def columns(c, carry):
            here = pl.ds(pl.multiple_of(c * wide, wide), wide)
            found = jnp.dot(chosen, source[:, here], preferred_element_type=jnp.float32)
            found = found.astype(jnp.bfloat16)
            if d == H:
                lo = way * (slots // 2)
                stage[j, lo : lo + slots // 2, here] = found[lo : lo + slots // 2, :]
            else:
                stage[j, :, here] = found
            return carry

        lax.fori_loop(0, width // wide, columns, 0)

    landed = set()

    def await_piece(d, p):
        if (d, p) not in landed:
            for way in range(2):
                passing(way, d, p).wait_recv()
            landed.add((d, p))

    def pass_on(d, p):
        for way in range(2):
            if p == 0 and d > 1:
                passing_meta(way, d - 1).wait_recv()
            if p == 0:
                passing_meta(way, d).start()
        if d > 1:
            await_piece(d - 1, p)
        for way in range(2):
            passing(way, d, p).start()

    def pick_plane(d):
        if d == H:
            for way in range(2):
                passing_meta(way, d).wait_recv()
        for p in range(plan.pieces[d]):
            await_piece(d, p)
        for way, j in places(d):
            pick(way, d, j)
        for j in spots(d):
            exchange(j, hand_over)

    def expert(j):
        hidden = []
        for half in range(2):
            gated = jnp.dot(arrived[j], wg[half], preferred_element_type=jnp.float32)
            upward = jnp.dot(arrived[j], wu[half], preferred_element_type=jnp.float32)
            hidden.append((gated / (1.0 + jnp.exp(-gated)) * upward).astype(jnp.bfloat16))
        step = min(256, width)

        def down(c, carry):
            here = pl.ds(pl.multiple_of(c * step, step), step)
            total = jnp.zeros((slots, step), jnp.float32)
            for half in range(2):
                part = lax.dot_general(
                    hidden[half], wd[half, here, :], (((1,), (1,)), ((), ())),
                    preferred_element_type=jnp.float32,
                )
                total = total + part.astype(jnp.bfloat16).astype(jnp.float32)
            arrived[j, :, here] = total.astype(jnp.bfloat16)
            return carry

        lax.fori_loop(0, width // step, down, 0)

    def compute(d, n):
        j = spots(d)[n]
        all_columns(j, arrived, xsend.at[0], xrecv.at[j]).wait_recv()
        expert(j)
        exchange(j, give_back)

    def prepare(way, d, j):
        n = rows if d == 0 else plan.prefix[d]
        meta = meta_ref[2] if d == 0 else metas[way, d - 1]
        w = hits(plan, meta, n, z, way, d, True)
        high = w.astype(jnp.bfloat16).astype(jnp.float32)
        spread[way, :n, :] = jnp.concatenate([high, w - high], axis=0).T.astype(jnp.bfloat16)
        doubled[way, :slots, :] = rows_in[j]
        doubled[way, slots:, :] = rows_in[j]

    def wait_rows(d):
        for j in spots(d):
            all_columns(j, rows_in, ysend.at[0], yrecv.at[j]).wait_recv()

    def hop_sent(way, d):
        here = ring.at[way, pl.ds(plan.offset[d], plan.prefix[d]), :]
        remote(here, here, zsend.at[way, d - 1], zrecv.at[way, 0], ep=outward[way]).wait_send()

    def combine(d):
        wait_rows(d)
        for way, j in places(d):
            prepare(way, d, j)
        if d < H:
            for way in range(2):
                hop_sent(way, d + 1)

        def one(p, carry, joined):
            for way in range(2):
                if joined:
                    closer(way, d + 1, p).wait_recv()
                place = spread[way, pl.ds(pl.multiple_of(p * piece, piece), piece), :]
                mine = pl.ds(pl.multiple_of(plan.offset[d] + p * piece, piece), piece)
                for c in range(0, width, wide):
                    part = jnp.dot(
                        place, doubled[way, :, c : c + wide], preferred_element_type=jnp.float32
                    )
                    if joined:
                        there = pl.ds(pl.multiple_of(plan.offset[d + 1] + p * piece, piece), piece)
                        part = part + back[way, there, c : c + wide].astype(jnp.float32)
                    ring[way, mine, c : c + wide] = part.astype(jnp.bfloat16)
            for way in range(2):
                closer(way, d, p).start()
            return carry

        old, new = plan.pieces[d + 1], plan.pieces[d]
        if new > old:
            lax.fori_loop(old, new, functools.partial(one, joined=False), 0)
        if old:
            lax.fori_loop(0, old, functools.partial(one, joined=True), 0)

    weights = []
    for i, (src, dst) in enumerate(((wg_ref, wg), (wu_ref, wu), (wd_ref, wd))):
        weights.append(remote(src, dst.at[1], wsend.at[i], wrecv.at[i], tp=other))
        weights.append(pltpu.make_async_copy(src, dst.at[0], wown.at[i]))
    for i, (kind, d, *which) in enumerate(schedule(plan)):
        if kind == "go":
            pass_on(d, *which)
        elif kind == "pick":
            pick_plane(d)
        elif kind == "expert":
            if d == 0:
                for copy in weights:
                    copy.wait()
            compute(d, *which)
        else:
            combine(d)
        if i == 2:
            for copy in weights:
                copy.start()

    wait_rows(0)
    prepare(0, 0, 0)
    order = []
    for way in range(2):
        slot = iota((rows, rows), 0).astype(jnp.float32)
        rank = meta_ref[2, 4 + way : 5 + way, :]
        order.append(jnp.where(slot == rank, 1.0, 0.0).T.astype(jnp.bfloat16))

        def arrive(p, carry, way=way):
            closer(way, 1, p).wait_recv()
            return carry

        lax.fori_loop(0, plan.pieces[1], arrive, 0)
    squares = jnp.zeros((rows, 1), jnp.float32)
    first = plan.offset[1]
    sums = []
    for c in range(0, width, wide):
        part = jnp.dot(spread[0], doubled[0, :, c : c + wide], preferred_element_type=jnp.float32)
        for way in range(2):
            part = part + jnp.dot(
                order[way], back[way, first : first + rows, c : c + wide],
                preferred_element_type=jnp.float32,
            )
        sums.append(part)
        squares = squares + jnp.sum(part * part, axis=1, keepdims=True)
    inverse = lax.rsqrt(squares / width + EPS)
    half_width = width // 2
    here = min(wide, half_width)
    for i, c in enumerate(range(0, width, wide)):
        scaled = (sums[i] * inverse).astype(jnp.bfloat16)
        for s in range(0, wide, here):
            halves[(c + s) // half_width, :, (c + s) % half_width : (c + s) % half_width + here] = (
                scaled[:, s : s + here]
            )
    mine = pl.ds(pl.multiple_of(core * rows, rows), rows)
    swap = remote(halves.at[other], final.at[mine, :], fsem.at[0], fsem.at[1], tp=other)
    swap.start()
    final[mine, :] = halves[core]

    sent = pl.ds(0, Z * (X - 1) // X)
    remote(stage.at[sent], stage.at[sent], xsend.at[0], xrecv.at[0], ep=outward[0]).wait_send()
    remote(arrived.at[sent], arrived.at[sent], ysend.at[0], yrecv.at[0], ep=outward[0]).wait_send()
    remote(metas, metas, msend.at[0], mrecv.at[0, 0], ep=outward[0]).wait_send()
    for way in range(2):
        hop_sent(way, 1)
        remote(
            ring.at[way], ring.at[way], bsend.at[way], brecv.at[way, 0], ep=homeward[way]
        ).wait_send()
    theirs = pl.ds(pl.multiple_of(other * rows, rows), rows)
    swap.wait_send()
    remote(halves.at[core], final.at[theirs, :], fsem.at[0], fsem.at[1], tp=other).wait_recv()
    out_ref[...] = (final[...].astype(jnp.float32) * gain_out_ref[...]).astype(jnp.bfloat16)


def run_experts(plan, tokens, gain_in, expert_ids, gate_weights, w_gate, w_up, w_down, gain_out):
    X, Z, H, rows, width = plan.X, plan.Z, plan.H, plan.rows, plan.width
    dma = pltpu.SemaphoreType.DMA
    hops = (2, sum(plan.pieces))
    bf16 = jnp.bfloat16
    return pl.pallas_call(
        functools.partial(experts_kernel, plan),
        out_shape=jax.ShapeDtypeStruct((2 * rows, width // 2), bf16),
        in_specs=[VMEM, VMEM, VMEM, VMEM, ANY, ANY, ANY, VMEM],
        out_specs=VMEM,
        scratch_shapes=[
            pltpu.VMEM((rows, width), bf16),
            pltpu.VMEM((rows, width), bf16),
            pltpu.VMEM((rows, width), bf16),
            pltpu.VMEM((3, 8, rows), jnp.float32),
            pltpu.VMEM((2, plan.total, width), bf16),
            pltpu.VMEM((2, plan.total, width), bf16),
            pltpu.VMEM((2, H, 8, rows), jnp.float32),
            pltpu.VMEM((Z, plan.slots, width), bf16),
            pltpu.VMEM((Z, plan.slots, width), bf16),
            pltpu.VMEM((Z, plan.slots, width), bf16),
            pltpu.VMEM((2, rows, 2 * plan.slots), bf16),
            pltpu.VMEM((2, 2 * plan.slots, width), bf16),
            pltpu.VMEM((2,) + w_gate.shape, bf16),
            pltpu.VMEM((2,) + w_up.shape, bf16),
            pltpu.VMEM((2,) + w_down.shape, bf16),
            pltpu.VMEM((2, rows, width // 2), bf16),
            pltpu.VMEM((2 * rows, width // 2), bf16),
            dma((2, H)), dma(hops), dma((2,)), dma(hops), dma((1,)), dma((2, H)),
            dma((1,)), dma((Z,)), dma((1,)), dma((Z,)),
            dma((3,)), dma((3,)), dma((3,)), dma((2,)),
        ],
        compiler_params=pltpu.CompilerParams(
            collective_id=0, has_side_effects=True, vmem_limit_bytes=VMEM_LIMIT
        ),
        name="run_experts",
    )(
        tokens, gain_in.reshape(1, width), expert_ids.T, gate_weights.T,
        w_gate, w_up, w_down, gain_out.reshape(1, width // 2),
    )


def per_device(columns, tokens, gain_in, expert_ids, gate_weights, w_gate, w_up, w_down, gain_out):
    own_rows, width = tokens.shape
    members = lax.axis_size("ep")
    capacity = 2 * own_rows * expert_ids.shape[1] // members
    plan = Plan(own_rows, width, members, capacity, columns)
    return run_experts(
        plan, tokens, gain_in, expert_ids, gate_weights, w_gate[0], w_up[0], w_down[0], gain_out
    )


def solution(mesh, columns=COLUMNS):
    placed = (
        P(("grp", "ep", "tp"), None),
        P(),
        P(("grp", "ep"), None),
        P(("grp", "ep"), None),
        P("ep", None, "tp"),
        P("ep", None, "tp"),
        P("ep", None, "tp"),
        P("tp"),
    )
    return jax.shard_map(
        functools.partial(per_device, columns),
        mesh=mesh, in_specs=placed, out_specs=P(("grp", "ep"), "tp"), check_vma=False,
    )
```

```python
import functools

import jax
import jax.numpy as jnp
from jax import lax
from jax.experimental import pallas as pl
from jax.experimental.pallas import tpu as pltpu
from jax.sharding import PartitionSpec as P

EPS = 1e-06
COLUMNS = 4
MESH = pl.DeviceIdType.MESH
VMEM = pl.BlockSpec(memory_space=pltpu.VMEM)
ANY = pl.BlockSpec(memory_space=pl.ANY)
VMEM_LIMIT = 60 * 1024 * 1024


class Plan:
    def __init__(self, rows, width, members, capacity, columns):
        self.rows, self.width, self.members, self.cap, self.X = rows, width, members, capacity, columns
        self.Z = members // columns
        self.H = self.Z // 2
        self.slots = columns * capacity
        self.piece = self.slots // 2
        self.prefix = [0] + [
            min(rows, (self.H - d) * self.slots + self.slots // 2) for d in range(1, self.H + 1)
        ] + [0]
        self.pieces = [n // self.piece for n in self.prefix]
        self.offset = [sum(self.prefix[:d]) for d in range(self.H + 2)]
        self.total = sum(self.prefix)
        self.most = max(self.pieces)

    def number(self, d, p):
        return self.offset[d] // self.piece + p

    def me(self):
        ep = lax.axis_index("ep")
        return ep // self.X, ep % self.X

    def at(self, z, x):
        return lax.rem(z + 2 * self.Z, self.Z) * self.X + lax.rem(x + 2 * self.X, self.X)


def remote(src, dst, send, recv, **where):
    return pltpu.make_async_remote_copy(
        src_ref=src, dst_ref=dst, send_sem=send, recv_sem=recv, device_id=where, device_id_type=MESH
    )


def greet(plan):
    z, x = plan.me()
    peers = [{"ep": plan.at(z + 1, x)}, {"ep": plan.at(z - 1, x)}]
    peers += [{"ep": plan.at(z, x + r)} for r in range(1, plan.X)]
    peers.append({"tp": 1 - lax.axis_index("tp")})
    barrier = pltpu.get_barrier_semaphore()
    for peer in peers:
        pl.semaphore_signal(barrier, inc=1, device_id=peer, device_id_type=MESH)
    return barrier, len(peers)


def iota(shape, dim):
    return lax.broadcasted_iota(jnp.int32, shape, dim)


def sort_tokens(plan, x_ref, gain_ref, ids_ref, gates_ref, own, orders, meta_ref, normed):
    rows, X, Z, H = plan.rows, plan.X, plan.Z, plan.H
    z, _ = plan.me()
    step = 32

    def norm_step(i, carry):
        here = pl.ds(pl.multiple_of(i * step, step), step)
        x = x_ref[here, :].astype(jnp.float32)
        scale = lax.rsqrt(jnp.mean(x * x, axis=1, keepdims=True) + EPS)
        normed[here, :] = (x * scale * gain_ref[...]).astype(jnp.bfloat16)
        return carry

    lax.fori_loop(0, rows // step, norm_step, 0)

    mine = pl.ds(pl.multiple_of(lax.axis_index("tp") * rows, rows), rows)
    square = (rows, rows)
    sub, lane = iota(square, 0), iota(square, 1)
    eye = sub == lane

    def as_column(row):
        return jnp.sum(jnp.where(eye, row, 0.0), axis=1, keepdims=True)

    def count(mask, axis):
        return jnp.sum(jnp.where(mask, 1.0, 0.0), axis=axis, keepdims=True)

    rws = [ids_ref[k : k + 1, mine].astype(jnp.float32) for k in range(2)]
    cols = [as_column(r) for r in rws]
    grws = [gates_ref[k : k + 1, mine] for k in range(2)]
    gcols = [as_column(g) for g in grws]
    q_col, q_row, key_col, key_row = [], [], [[], []], [[], []]
    for k in range(2):
        slot_row = count((sub < lane) & (cols[0] == rws[k]), 0) + count((sub < lane) & (cols[1] == rws[k]), 0)
        slot_col = count((lane < sub) & (rws[0] == cols[k]), 1) + count((lane < sub) & (rws[1] == cols[k]), 1)
        q_row.append(rws[k] * plan.cap + slot_row)
        q_col.append(cols[k] * plan.cap + slot_col)
        for expert, keys in ((rws[k], key_row), (cols[k], key_col)):
            e = expert.astype(jnp.int32)
            ahead = e // X - z
            ahead = jnp.where(ahead < 0, ahead + Z, ahead)
            first = e % X < X // 2
            up = jnp.where((ahead < H) | ((ahead == H) & first), ahead, 0)
            down = jnp.where((ahead > H) | ((ahead == H) & ~first), Z - ahead, 0)
            keys[0].append(up.astype(jnp.float32))
            keys[1].append(down.astype(jnp.float32))
    for k in range(2):
        meta_ref[2, k : k + 1, :] = q_row[k]
        meta_ref[2, 2 + k : 3 + k, :] = grws[k]
    for way in range(2):
        far_col = jnp.maximum(*key_col[way])
        far_row = jnp.maximum(*key_row[way])
        rank_row = count((far_col > far_row) | ((far_col == far_row) & (sub < lane)), 0)
        rank_col = count((far_row > far_col) | ((far_row == far_col) & (lane < sub)), 1)
        meta_ref[2, 4 + way : 5 + way, :] = rank_row
        chosen = rank_col == lane.astype(jnp.float32)
        for k in range(2):
            meta_ref[way, k : k + 1, :] = jnp.sum(jnp.where(chosen, q_col[k], 0.0), axis=0, keepdims=True)
            meta_ref[way, 2 + k : 3 + k, :] = jnp.sum(jnp.where(chosen, gcols[k], 0.0), axis=0, keepdims=True)
        meta_ref[way, 4:8, :] = jnp.zeros((4, rows), jnp.float32)
        orders[way] = jnp.where(sub.astype(jnp.float32) == rank_row, 1.0, 0.0).astype(jnp.bfloat16)
    meta_ref[2, 6:8, :] = jnp.zeros((2, rows), jnp.float32)

    def write(lo, hi):
        n = min(512, plan.width)
        for way in range(2):
            for c in range(0, plan.width, n):
                own[way][lo:hi, c : c + n] = jnp.dot(
                    orders[way, lo:hi, :], normed[:, c : c + n], preferred_element_type=jnp.float32
                ).astype(jnp.bfloat16)

    return write


def hits(plan, meta, n, z, way, d, weighted):
    slots, cap = plan.slots, plan.cap
    slot = iota((slots, n), 0)
    base = z * slots
    total = jnp.zeros((slots, n), jnp.float32)
    for k in range(2):
        match = meta[k : k + 1, :n].astype(jnp.int32) - base == slot
        if d == plan.H:
            match = match & (slot < slots // 2 if way == 0 else slot >= slots // 2)
        total = total + jnp.where(match, meta[2 + k : 3 + k, :n] if weighted else 1.0, 0.0)
    return total


def schedule(plan):
    if plan.pieces != [0, 8, 8, 8, 8, 7, 5, 3, 1, 0]:
        raise ValueError("no schedule")

    def go(*pieces):
        return [("go", d, p) for d, p in pieces]

    def expert(d):
        return [("expert", d, 0), ("expert", d, 1)]

    def first(d):
        return go((d, 0), (d, 1), (d, 2))

    return (
        first(1) + [("pick", 0)] + first(2) + first(3) + first(4) + [("expert", 0, 0)]
        + first(5) + first(6) + first(7)
        + go((1, 3), (8, 0), (1, 4), (1, 5)) + [("pick", 7)]
        + go((2, 3), (2, 4), (1, 6)) + [("pick", 8)]
        + go((3, 3), (3, 4), (2, 5)) + [("expert", 7, 0)]
        + go((4, 3), (4, 4), (2, 6)) + [("expert", 7, 1)]
        + go((5, 3), (5, 4), (3, 5)) + [("expert", 8, 0)]
        + go((6, 3), (6, 4), (3, 6), (1, 7), (4, 5), (4, 6)) + [("pick", 6)]
        + go((2, 7), (5, 5), (5, 6)) + expert(6)
        + go((3, 7)) + [("sum", 8), ("pick", 5), ("sum", 7)]
        + go((4, 7)) + expert(5) + [("sum", 6), ("pick", 4), ("pick", 3), ("sum", 5)]
        + expert(4) + expert(3) + [("sum", 4), ("pick", 2), ("pick", 1)]
        + expert(2) + [("sum", 3)] + expert(1) + [("sum", 2), ("sum", 1)]
    )


def experts_kernel(
    plan,
    x_ref, gain_ref, ids_ref, gates_ref, wg_ref, wu_ref, wd_ref, gain_out_ref,
    out_ref,
    normed, plus_ref, minus_ref, meta_ref, ring, back, metas, stage, arrived, rows_in, spread, doubled,
    wg, wu, wd, halves, final, orders, unsort, gathered,
    zsend, zrecv, bsend, brecv, msend, mrecv, xsend, xrecv, ysend, yrecv,
    wsend, wrecv, wown, fsend, frecv, osem,
):
    X, Z, H, cap, piece = plan.X, plan.Z, plan.H, plan.cap, plan.piece
    rows, width, slots = plan.rows, plan.width, plan.slots
    wide = min(512, width)
    z, x = plan.me()
    core = lax.axis_index("tp")
    other = 1 - core
    barrier, peers = greet(plan)
    own = (plus_ref, minus_ref)
    write = sort_tokens(plan, x_ref, gain_ref, ids_ref, gates_ref, own, orders, meta_ref, normed)
    lead = 3 * piece
    write(0, lead)
    pl.semaphore_wait(barrier, peers)

    outward = (plan.at(z + 1, x), plan.at(z - 1, x))
    homeward = (outward[1], outward[0])
    def places(d):
        if d == 0:
            return [(0, 0)]
        if d == H:
            return [(0, Z - 1), (1, Z - 1)]
        return [(0, 2 * d - 1), (1, 2 * d)]

    def spots(d):
        return sorted({j for _, j in places(d)})

    def passing(way, d, p):
        dst = ring.at[way, pl.ds(plan.offset[d] + p * piece, piece), :]
        if d == 1:
            src = own[way].at[pl.ds(p * piece, piece), :]
        else:
            src = ring.at[way, pl.ds(plan.offset[d - 1] + p * piece, piece), :]
        return remote(src, dst, zsend.at[way, d - 1], zrecv.at[way, plan.number(d, p)], ep=outward[way])

    def passing_meta(way, d):
        src = meta_ref.at[way] if d == 1 else metas.at[way, d - 2]
        return remote(src, metas.at[way, d - 1], msend.at[0], mrecv.at[way, d - 1], ep=outward[way])

    def closer(way, d, p):
        here = pl.ds(plan.offset[d] + p * piece, piece)
        return remote(
            ring.at[way, here, :], back.at[way, here, :],
            bsend.at[way], brecv.at[way, plan.number(d, p)], ep=homeward[way],
        )

    def column(r):
        return pl.ds(pl.multiple_of(lax.rem(x + r, X) * cap, cap), cap)

    def hand_over(j, r):
        src, dst = stage.at[j, column(r), :], arrived.at[j, column(0), :]
        return remote(src, dst, xsend.at[0], xrecv.at[j], ep=plan.at(z, x + r))

    def give_back(j, r):
        src, dst = arrived.at[j, column(r), :], rows_in.at[j, column(0), :]
        return remote(src, dst, ysend.at[0], yrecv.at[j], ep=plan.at(z, x + r))

    def all_columns(j, ref, send, recv):
        part = ref.at[j, pl.ds(0, plan.slots - cap), :]
        return remote(part, part, send, recv, ep=plan.at(z, x + 1))

    def exchange(j, copy):
        for r in range(1, X):
            copy(j, r).start()
        if copy is hand_over:
            arrived[j, column(0), :] = stage[j, column(0), :]
        else:
            rows_in[j, column(0), :] = arrived[j, column(0), :]

    def pick(way, d, j):
        n = rows if d == 0 else plan.prefix[d]
        meta = meta_ref[0] if d == 0 else metas[way, d - 1]
        source = plus_ref if d == 0 else ring.at[way, pl.ds(plan.offset[d], n), :]
        chosen = hits(plan, meta, n, z, way, d, False).astype(jnp.bfloat16)

        def columns(c, carry):
            here = pl.ds(pl.multiple_of(c * wide, wide), wide)
            found = jnp.dot(chosen, source[:, here], preferred_element_type=jnp.float32)
            found = found.astype(jnp.bfloat16)
            if d == H:
                lo = way * (slots // 2)
                stage[j, lo : lo + slots // 2, here] = found[lo : lo + slots // 2, :]
            else:
                stage[j, :, here] = found
            return carry

        lax.fori_loop(0, width // wide, columns, 0)

    landed = set()

    def await_piece(d, p):
        if (d, p) not in landed:
            for way in range(2):
                passing(way, d, p).wait_recv()
            landed.add((d, p))

    def pass_on(d, p):
        for way in range(2):
            if p == 0 and d > 1:
                passing_meta(way, d - 1).wait_recv()
            if p == 0:
                passing_meta(way, d).start()
        if d > 1:
            await_piece(d - 1, p)
        for way in range(2):
            passing(way, d, p).start()

    def pick_plane(d):
        if d == H:
            for way in range(2):
                passing_meta(way, d).wait_recv()
        for p in range(plan.pieces[d]):
            await_piece(d, p)
        for way, j in places(d):
            pick(way, d, j)
        for j in spots(d):
            exchange(j, hand_over)

    def expert(j):
        hidden = []
        for half in range(2):
            gated = jnp.dot(arrived[j], wg[half], preferred_element_type=jnp.float32)
            upward = jnp.dot(arrived[j], wu[half], preferred_element_type=jnp.float32)
            hidden.append((gated / (1.0 + jnp.exp(-gated)) * upward).astype(jnp.bfloat16))
        step = min(256, width)

        def down(c, carry):
            here = pl.ds(pl.multiple_of(c * step, step), step)
            total = jnp.zeros((slots, step), jnp.float32)
            for half in range(2):
                part = lax.dot_general(
                    hidden[half], wd[half, here, :], (((1,), (1,)), ((), ())),
                    preferred_element_type=jnp.float32,
                )
                total = total + part.astype(jnp.bfloat16).astype(jnp.float32)
            arrived[j, :, here] = total.astype(jnp.bfloat16)
            return carry

        lax.fori_loop(0, width // step, down, 0)

    def compute(d, n):
        j = spots(d)[n]
        all_columns(j, arrived, xsend.at[0], xrecv.at[j]).wait_recv()
        expert(j)
        exchange(j, give_back)

    def prepare(way, d, j):
        n = rows if d == 0 else plan.prefix[d]
        meta = meta_ref[2] if d == 0 else metas[way, d - 1]
        w = hits(plan, meta, n, z, way, d, True)
        high = w.astype(jnp.bfloat16).astype(jnp.float32)
        spread[way, :n, :] = jnp.concatenate([high, w - high], axis=0).T.astype(jnp.bfloat16)
        doubled[way, :slots, :] = rows_in[j]
        doubled[way, slots:, :] = rows_in[j]

    def wait_rows(d):
        for j in spots(d):
            all_columns(j, rows_in, ysend.at[0], yrecv.at[j]).wait_recv()

    def hop_sent(way, d):
        here = ring.at[way, pl.ds(plan.offset[d], plan.prefix[d]), :]
        remote(here, here, zsend.at[way, d - 1], zrecv.at[way, 0], ep=outward[way]).wait_send()

    def combine(d):
        wait_rows(d)
        for way, j in places(d):
            prepare(way, d, j)
        if d < H:
            for way in range(2):
                hop_sent(way, d + 1)

        def one(p, carry, joined):
            for way in range(2):
                if joined:
                    closer(way, d + 1, p).wait_recv()
                place = spread[way, pl.ds(pl.multiple_of(p * piece, piece), piece), :]
                mine = pl.ds(pl.multiple_of(plan.offset[d] + p * piece, piece), piece)
                for c in range(0, width, wide):
                    part = jnp.dot(
                        place, doubled[way, :, c : c + wide], preferred_element_type=jnp.float32
                    )
                    if joined:
                        there = pl.ds(pl.multiple_of(plan.offset[d + 1] + p * piece, piece), piece)
                        part = part + back[way, there, c : c + wide].astype(jnp.float32)
                    ring[way, mine, c : c + wide] = part.astype(jnp.bfloat16)
            for way in range(2):
                closer(way, d, p).start()
            return carry

        old, new = plan.pieces[d + 1], plan.pieces[d]
        if new > old:
            lax.fori_loop(old, new, functools.partial(one, joined=False), 0)
        if old:
            lax.fori_loop(0, old, functools.partial(one, joined=True), 0)

    def own_rows():
        wait_rows(0)
        prepare(0, 0, 0)
        for c in range(0, width, wide):
            gathered[:, c : c + wide] = jnp.dot(
                spread[0], doubled[0, :, c : c + wide], preferred_element_type=jnp.float32
            )
        for way in range(2):
            slot = iota((rows, rows), 0).astype(jnp.float32)
            rank = meta_ref[2, 4 + way : 5 + way, :]
            unsort[way] = jnp.where(slot == rank, 1.0, 0.0).T.astype(jnp.bfloat16)

    weights = []
    for i, (src, dst) in enumerate(((wg_ref, wg), (wu_ref, wu), (wd_ref, wd))):
        weights.append(remote(src, dst.at[1], wsend.at[i], wrecv.at[i], tp=other))
        weights.append(pltpu.make_async_copy(src, dst.at[0], wown.at[i]))
    for i, (kind, d, *which) in enumerate(schedule(plan)):
        if kind == "go":
            pass_on(d, *which)
        elif kind == "pick":
            pick_plane(d)
        elif kind == "expert":
            if d == 0:
                for copy in weights:
                    copy.wait()
            compute(d, *which)
        else:
            if d == 1:
                own_rows()
            combine(d)
        if i == 2:
            write(lead, rows)
            for copy in weights:
                copy.start()

    first, end = plan.offset[1], plan.offset[1] + rows
    early = end - piece
    for way in range(2):
        def arrive(p, carry, way=way):
            closer(way, 1, p).wait_recv()
            return carry

        lax.fori_loop(0, plan.pieces[1] - 1, arrive, 0)
    for c in range(0, width, wide):
        part = gathered[:, c : c + wide]
        for way in range(2):
            part = part + jnp.dot(
                unsort[way, :, : rows - piece], back[way, first:early, c : c + wide],
                preferred_element_type=jnp.float32,
            )
        gathered[:, c : c + wide] = part
    for way in range(2):
        closer(way, 1, plan.pieces[1] - 1).wait_recv()
    gain = gain_out_ref[...]
    half_width, some = width // 2, rows // 2
    here = min(wide, half_width)

    def swap(i):
        src = halves.at[other, pl.ds(i * some, some), :]
        return remote(src, final.at[1, pl.ds(i * some, some), :], fsend.at[i], frecv.at[i], tp=other)

    def put(i, who):
        at = pl.ds(pl.multiple_of((core if who == 0 else other) * rows + i * some, some), some)
        return pltpu.make_async_copy(
            final.at[2 * who, pl.ds(i * some, some), :], out_ref.at[at, :], osem.at[who, i]
        )

    for i in range(2):
        part_rows = slice(i * some, (i + 1) * some)
        squares = jnp.zeros((some, 1), jnp.float32)
        for c in range(0, width, wide):
            part = gathered[part_rows, c : c + wide]
            for way in range(2):
                part = part + jnp.dot(
                    unsort[way, part_rows, rows - piece :], back[way, early:end, c : c + wide],
                    preferred_element_type=jnp.float32,
                )
            gathered[part_rows, c : c + wide] = part
            squares = squares + jnp.sum(part * part, axis=1, keepdims=True)
        inverse = lax.rsqrt(squares / width + EPS)
        for c in range(0, width, here):
            halves[c // half_width, part_rows, c % half_width : c % half_width + here] = (
                gathered[part_rows, c : c + here] * inverse
            ).astype(jnp.bfloat16)
        swap(i).start()
    for i in range(2):
        part_rows = slice(i * some, (i + 1) * some)
        final[0, part_rows, :] = (
            halves[core, part_rows, :].astype(jnp.float32) * gain
        ).astype(jnp.bfloat16)
        put(i, 0).start()

    sent = pl.ds(0, Z * (X - 1) // X)
    remote(stage.at[sent], stage.at[sent], xsend.at[0], xrecv.at[0], ep=outward[0]).wait_send()
    remote(arrived.at[sent], arrived.at[sent], ysend.at[0], yrecv.at[0], ep=outward[0]).wait_send()
    remote(metas, metas, msend.at[0], mrecv.at[0, 0], ep=outward[0]).wait_send()
    for way in range(2):
        hop_sent(way, 1)
        remote(
            ring.at[way], ring.at[way], bsend.at[way], brecv.at[way, 0], ep=homeward[way]
        ).wait_send()
    for i in range(2):
        part_rows = slice(i * some, (i + 1) * some)
        swap(i).wait_recv()
        final[2, part_rows, :] = (
            final[1, part_rows, :].astype(jnp.float32) * gain
        ).astype(jnp.bfloat16)
        put(i, 1).start()
    for i in range(2):
        swap(i).wait_send()
        for who in range(2):
            put(i, who).wait()


def run_experts(plan, tokens, gain_in, expert_ids, gate_weights, w_gate, w_up, w_down, gain_out):
    X, Z, H, rows, width = plan.X, plan.Z, plan.H, plan.rows, plan.width
    dma = pltpu.SemaphoreType.DMA
    hops = (2, sum(plan.pieces))
    bf16 = jnp.bfloat16
    return pl.pallas_call(
        functools.partial(experts_kernel, plan),
        out_shape=jax.ShapeDtypeStruct((2 * rows, width // 2), bf16),
        in_specs=[VMEM, VMEM, VMEM, VMEM, ANY, ANY, ANY, VMEM],
        out_specs=ANY,
        scratch_shapes=[
            pltpu.VMEM((rows, width), bf16),
            pltpu.VMEM((rows, width), bf16),
            pltpu.VMEM((rows, width), bf16),
            pltpu.VMEM((3, 8, rows), jnp.float32),
            pltpu.VMEM((2, plan.total, width), bf16),
            pltpu.VMEM((2, plan.total, width), bf16),
            pltpu.VMEM((2, H, 8, rows), jnp.float32),
            pltpu.VMEM((Z, plan.slots, width), bf16),
            pltpu.VMEM((Z, plan.slots, width), bf16),
            pltpu.VMEM((Z, plan.slots, width), bf16),
            pltpu.VMEM((2, rows, 2 * plan.slots), bf16),
            pltpu.VMEM((2, 2 * plan.slots, width), bf16),
            pltpu.VMEM((2,) + w_gate.shape, bf16),
            pltpu.VMEM((2,) + w_up.shape, bf16),
            pltpu.VMEM((2,) + w_down.shape, bf16),
            pltpu.VMEM((2, rows, width // 2), bf16),
            pltpu.VMEM((3, rows, width // 2), bf16),
            pltpu.VMEM((2, rows, rows), bf16),
            pltpu.VMEM((2, rows, rows), bf16),
            pltpu.VMEM((rows, width), jnp.float32),
            dma((2, H)), dma(hops), dma((2,)), dma(hops), dma((1,)), dma((2, H)),
            dma((1,)), dma((Z,)), dma((1,)), dma((Z,)),
            dma((3,)), dma((3,)), dma((3,)), dma((2,)), dma((2,)), dma((2, 2)),
        ],
        compiler_params=pltpu.CompilerParams(
            collective_id=0, has_side_effects=True, vmem_limit_bytes=VMEM_LIMIT
        ),
        name="run_experts",
    )(
        tokens, gain_in.reshape(1, width), expert_ids.T, gate_weights.T,
        w_gate, w_up, w_down, gain_out.reshape(1, width // 2),
    )


def per_device(columns, tokens, gain_in, expert_ids, gate_weights, w_gate, w_up, w_down, gain_out):
    own_rows, width = tokens.shape
    members = lax.axis_size("ep")
    capacity = 2 * own_rows * expert_ids.shape[1] // members
    plan = Plan(own_rows, width, members, capacity, columns)
    return run_experts(
        plan, tokens, gain_in, expert_ids, gate_weights, w_gate[0], w_up[0], w_down[0], gain_out
    )


def solution(mesh, columns=COLUMNS):
    placed = (
        P(("grp", "ep", "tp"), None),
        P(),
        P(("grp", "ep"), None),
        P(("grp", "ep"), None),
        P("ep", None, "tp"),
        P("ep", None, "tp"),
        P("ep", None, "tp"),
        P("tp"),
    )
    return jax.shard_map(
        functools.partial(per_device, columns),
        mesh=mesh, in_specs=placed, out_specs=P(("grp", "ep"), "tp"), check_vma=False,
    )
```

```python
import functools

import jax
import jax.numpy as jnp
from jax import lax
from jax.experimental import pallas as pl
from jax.experimental.pallas import tpu as pltpu
from jax.sharding import PartitionSpec as P

EPS = 1e-06
COLUMNS = 4
MESH = pl.DeviceIdType.MESH
VMEM = pl.BlockSpec(memory_space=pltpu.VMEM)
ANY = pl.BlockSpec(memory_space=pl.ANY)
VMEM_LIMIT = 60 * 1024 * 1024


class Plan:
    def __init__(self, rows, width, members, capacity, columns):
        self.rows, self.width, self.members, self.cap, self.X = rows, width, members, capacity, columns
        self.Z = members // columns
        self.H = self.Z // 2
        self.slots = columns * capacity
        self.piece = self.slots // 2
        self.prefix = [0] + [
            min(rows, (self.H - d) * self.slots + self.slots // 2) for d in range(1, self.H + 1)
        ] + [0]
        self.pieces = [n // self.piece for n in self.prefix]
        self.offset = [sum(self.prefix[:d]) for d in range(self.H + 2)]
        self.total = sum(self.prefix)
        self.most = max(self.pieces)

    def number(self, d, p):
        return self.offset[d] // self.piece + p

    def me(self):
        ep = lax.axis_index("ep")
        return ep // self.X, ep % self.X

    def at(self, z, x):
        return lax.rem(z + 2 * self.Z, self.Z) * self.X + lax.rem(x + 2 * self.X, self.X)


def remote(src, dst, send, recv, **where):
    return pltpu.make_async_remote_copy(
        src_ref=src, dst_ref=dst, send_sem=send, recv_sem=recv, device_id=where, device_id_type=MESH
    )


def greet(plan):
    z, x = plan.me()
    peers = [{"ep": plan.at(z + 1, x)}, {"ep": plan.at(z - 1, x)}]
    peers += [{"ep": plan.at(z, x + r)} for r in range(1, plan.X)]
    peers.append({"tp": 1 - lax.axis_index("tp")})
    barrier = pltpu.get_barrier_semaphore()
    for peer in peers:
        pl.semaphore_signal(barrier, inc=1, device_id=peer, device_id_type=MESH)
    return barrier, len(peers)


def iota(shape, dim):
    return lax.broadcasted_iota(jnp.int32, shape, dim)


def sort_tokens(plan, x_ref, gain_ref, ids_ref, gates_ref, own, orders, meta_ref, normed):
    rows, X, Z, H = plan.rows, plan.X, plan.Z, plan.H
    z, _ = plan.me()
    step = 32

    def norm_step(i, carry):
        here = pl.ds(pl.multiple_of(i * step, step), step)
        x = x_ref[here, :].astype(jnp.float32)
        scale = lax.rsqrt(jnp.mean(x * x, axis=1, keepdims=True) + EPS)
        normed[here, :] = (x * scale * gain_ref[...]).astype(jnp.bfloat16)
        return carry

    lax.fori_loop(0, rows // step, norm_step, 0)

    mine = pl.ds(pl.multiple_of(lax.axis_index("tp") * rows, rows), rows)
    square = (rows, rows)
    sub, lane = iota(square, 0), iota(square, 1)
    eye = sub == lane

    def as_column(row):
        return jnp.sum(jnp.where(eye, row, 0.0), axis=1, keepdims=True)

    def count(mask, axis):
        return jnp.sum(jnp.where(mask, 1.0, 0.0), axis=axis, keepdims=True)

    rws = [ids_ref[k : k + 1, mine].astype(jnp.float32) for k in range(2)]
    cols = [as_column(r) for r in rws]
    grws = [gates_ref[k : k + 1, mine] for k in range(2)]
    gcols = [as_column(g) for g in grws]
    q_col, q_row, key_col, key_row = [], [], [[], []], [[], []]
    for k in range(2):
        slot_row = count((sub < lane) & (cols[0] == rws[k]), 0) + count((sub < lane) & (cols[1] == rws[k]), 0)
        slot_col = count((lane < sub) & (rws[0] == cols[k]), 1) + count((lane < sub) & (rws[1] == cols[k]), 1)
        q_row.append(rws[k] * plan.cap + slot_row)
        q_col.append(cols[k] * plan.cap + slot_col)
        for expert, keys in ((rws[k], key_row), (cols[k], key_col)):
            e = expert.astype(jnp.int32)
            ahead = e // X - z
            ahead = jnp.where(ahead < 0, ahead + Z, ahead)
            first = e % X < X // 2
            up = jnp.where((ahead < H) | ((ahead == H) & first), ahead, 0)
            down = jnp.where((ahead > H) | ((ahead == H) & ~first), Z - ahead, 0)
            keys[0].append(up.astype(jnp.float32))
            keys[1].append(down.astype(jnp.float32))
    for k in range(2):
        meta_ref[2, k : k + 1, :] = q_row[k]
        meta_ref[2, 2 + k : 3 + k, :] = grws[k]
    for way in range(2):
        far_col = jnp.maximum(*key_col[way])
        far_row = jnp.maximum(*key_row[way])
        rank_row = count((far_col > far_row) | ((far_col == far_row) & (sub < lane)), 0)
        rank_col = count((far_row > far_col) | ((far_row == far_col) & (lane < sub)), 1)
        meta_ref[2, 4 + way : 5 + way, :] = rank_row
        chosen = rank_col == lane.astype(jnp.float32)
        for k in range(2):
            meta_ref[way, k : k + 1, :] = jnp.sum(jnp.where(chosen, q_col[k], 0.0), axis=0, keepdims=True)
            meta_ref[way, 2 + k : 3 + k, :] = jnp.sum(jnp.where(chosen, gcols[k], 0.0), axis=0, keepdims=True)
        meta_ref[way, 4:8, :] = jnp.zeros((4, rows), jnp.float32)
        orders[way] = jnp.where(sub.astype(jnp.float32) == rank_row, 1.0, 0.0).astype(jnp.bfloat16)
    meta_ref[2, 6:8, :] = jnp.zeros((2, rows), jnp.float32)

    def write(lo, hi):
        n = min(512, plan.width)
        for way in range(2):
            for c in range(0, plan.width, n):
                own[way][lo:hi, c : c + n] = jnp.dot(
                    orders[way, lo:hi, :], normed[:, c : c + n], preferred_element_type=jnp.float32
                ).astype(jnp.bfloat16)

    return write


def hits(plan, meta, n, z, way, d, weighted):
    slots, cap = plan.slots, plan.cap
    slot = iota((slots, n), 0)
    base = z * slots
    total = jnp.zeros((slots, n), jnp.float32)
    for k in range(2):
        match = meta[k : k + 1, :n].astype(jnp.int32) - base == slot
        if d == plan.H:
            match = match & (slot < slots // 2 if way == 0 else slot >= slots // 2)
        total = total + jnp.where(match, meta[2 + k : 3 + k, :n] if weighted else 1.0, 0.0)
    return total


def schedule(plan):
    if plan.pieces != [0, 8, 8, 8, 8, 7, 5, 3, 1, 0]:
        raise ValueError("no schedule")

    def go(*pieces):
        return [("go", d, p) for d, p in pieces]

    def expert(d):
        return [("expert", d, 0), ("expert", d, 1)]

    def first(d):
        return go((d, 0), (d, 1), (d, 2))

    return (
        first(1) + [("pick", 0)] + first(2) + first(3) + first(4) + [("expert", 0, 0)]
        + first(5) + first(6) + first(7)
        + go((1, 3), (8, 0), (1, 4), (1, 5)) + [("pick", 7)]
        + go((2, 3), (2, 4), (1, 6)) + [("pick", 8)]
        + go((3, 3), (3, 4), (2, 5)) + [("expert", 7, 0)]
        + go((4, 3), (4, 4), (2, 6)) + [("expert", 7, 1)]
        + go((5, 3), (5, 4), (3, 5)) + [("expert", 8, 0)]
        + go((6, 3), (6, 4), (3, 6), (1, 7), (4, 5), (4, 6)) + [("pick", 6)]
        + go((2, 7), (5, 5), (5, 6)) + expert(6)
        + go((3, 7)) + [("sum", 8), ("pick", 5), ("sum", 7)]
        + go((4, 7)) + expert(5) + [("sum", 6), ("pick", 4), ("pick", 3), ("sum", 5)]
        + expert(4) + expert(3) + [("sum", 4), ("pick", 2), ("pick", 1)]
        + expert(2) + [("sum", 3)] + expert(1) + [("sum", 2), ("sum", 1)]
    )


def experts_kernel(
    plan,
    x_ref, gain_ref, ids_ref, gates_ref, wg_ref, wu_ref, wd_ref,
    out_ref,
    normed, plus_ref, minus_ref, meta_ref, ring, back, metas, stage, arrived, rows_in, spread, doubled,
    wg, wu, wd, halves, orders, unsort, gathered,
    zsend, zrecv, bsend, msend, mrecv, xsend, xrecv, ysend, yrecv,
    wsend, wrecv, wown, fsend, frecv, osem,
):
    X, Z, H, cap, piece = plan.X, plan.Z, plan.H, plan.cap, plan.piece
    rows, width, slots = plan.rows, plan.width, plan.slots
    wide = min(512, width)
    z, x = plan.me()
    core = lax.axis_index("tp")
    other = 1 - core
    barrier, peers = greet(plan)
    own = (plus_ref, minus_ref)
    write = sort_tokens(plan, x_ref, gain_ref, ids_ref, gates_ref, own, orders, meta_ref, normed)
    lead = 3 * piece
    write(0, lead)
    pl.semaphore_wait(barrier, peers)

    outward = (plan.at(z + 1, x), plan.at(z - 1, x))
    homeward = (outward[1], outward[0])
    def places(d):
        if d == 0:
            return [(0, 0)]
        if d == H:
            return [(0, Z - 1), (1, Z - 1)]
        return [(0, 2 * d - 1), (1, 2 * d)]

    def spots(d):
        return sorted({j for _, j in places(d)})

    def passing(way, d, p):
        dst = ring.at[way, pl.ds(plan.offset[d] + p * piece, piece), :]
        if d == 1:
            src = own[way].at[pl.ds(p * piece, piece), :]
        else:
            src = ring.at[way, pl.ds(plan.offset[d - 1] + p * piece, piece), :]
        return remote(src, dst, zsend.at[way, d - 1], zrecv.at[way, plan.number(d, p)], ep=outward[way])

    def passing_meta(way, d):
        src = meta_ref.at[way] if d == 1 else metas.at[way, d - 2]
        return remote(src, metas.at[way, d - 1], msend.at[0], mrecv.at[way, d - 1], ep=outward[way])

    def back_sem(way, d, p):
        return zrecv.at[way, plan.number(d - 1, p) if d > 1 else sum(plan.pieces) + p]

    def closer(way, d, p):
        here = pl.ds(plan.offset[d] + p * piece, piece)
        return remote(
            ring.at[way, here, :], back.at[way, here, :],
            bsend.at[way], back_sem(way, d, p), ep=homeward[way],
        )

    def column(r):
        return pl.ds(pl.multiple_of(lax.rem(x + r, X) * cap, cap), cap)

    def hand_over(j, r):
        src, dst = stage.at[j, column(r), :], arrived.at[j, column(0), :]
        return remote(src, dst, xsend.at[0], xrecv.at[j], ep=plan.at(z, x + r))

    def give_back(j, r):
        src, dst = arrived.at[j, column(r), :], rows_in.at[j, column(0), :]
        return remote(src, dst, ysend.at[0], yrecv.at[j], ep=plan.at(z, x + r))

    def all_columns(j, ref, send, recv):
        part = ref.at[j, pl.ds(0, plan.slots - cap), :]
        return remote(part, part, send, recv, ep=plan.at(z, x + 1))

    def exchange(j, copy):
        for r in range(1, X):
            copy(j, r).start()
        if copy is hand_over:
            arrived[j, column(0), :] = stage[j, column(0), :]
        else:
            rows_in[j, column(0), :] = arrived[j, column(0), :]

    def pick(way, d, j):
        n = rows if d == 0 else plan.prefix[d]
        meta = meta_ref[0] if d == 0 else metas[way, d - 1]
        source = plus_ref if d == 0 else ring.at[way, pl.ds(plan.offset[d], n), :]
        chosen = hits(plan, meta, n, z, way, d, False).astype(jnp.bfloat16)

        def columns(c, carry):
            here = pl.ds(pl.multiple_of(c * wide, wide), wide)
            found = jnp.dot(chosen, source[:, here], preferred_element_type=jnp.float32)
            found = found.astype(jnp.bfloat16)
            if d == H:
                lo = way * (slots // 2)
                stage[j, lo : lo + slots // 2, here] = found[lo : lo + slots // 2, :]
            else:
                stage[j, :, here] = found
            return carry

        lax.fori_loop(0, width // wide, columns, 0)

    landed = set()

    def await_piece(d, p):
        if (d, p) not in landed:
            for way in range(2):
                passing(way, d, p).wait_recv()
            landed.add((d, p))

    def pass_on(d, p):
        for way in range(2):
            if p == 0 and d > 1:
                passing_meta(way, d - 1).wait_recv()
            if p == 0:
                passing_meta(way, d).start()
        if d > 1:
            await_piece(d - 1, p)
        for way in range(2):
            passing(way, d, p).start()

    def pick_plane(d):
        if d == H:
            for way in range(2):
                passing_meta(way, d).wait_recv()
        for p in range(plan.pieces[d]):
            await_piece(d, p)
        for way, j in places(d):
            pick(way, d, j)
        for j in spots(d):
            exchange(j, hand_over)

    def expert(j):
        hidden = []
        for half in range(2):
            gated = jnp.dot(arrived[j], wg[half], preferred_element_type=jnp.float32)
            upward = jnp.dot(arrived[j], wu[half], preferred_element_type=jnp.float32)
            hidden.append((gated / (1.0 + jnp.exp(-gated)) * upward).astype(jnp.bfloat16))
        step = min(256, width)

        def down(c, carry):
            here = pl.ds(pl.multiple_of(c * step, step), step)
            total = jnp.zeros((slots, step), jnp.float32)
            for half in range(2):
                part = lax.dot_general(
                    hidden[half], wd[half, here, :], (((1,), (1,)), ((), ())),
                    preferred_element_type=jnp.float32,
                )
                total = total + part.astype(jnp.bfloat16).astype(jnp.float32)
            arrived[j, :, here] = total.astype(jnp.bfloat16)
            return carry

        lax.fori_loop(0, width // step, down, 0)

    def compute(d, n):
        j = spots(d)[n]
        all_columns(j, arrived, xsend.at[0], xrecv.at[j]).wait_recv()
        expert(j)
        exchange(j, give_back)

    def prepare(way, d, j):
        n = rows if d == 0 else plan.prefix[d]
        meta = meta_ref[2] if d == 0 else metas[way, d - 1]
        w = hits(plan, meta, n, z, way, d, True)
        high = w.astype(jnp.bfloat16).astype(jnp.float32)
        spread[way, :n, :] = jnp.concatenate([high, w - high], axis=0).T.astype(jnp.bfloat16)
        doubled[way, :slots, :] = rows_in[j]
        doubled[way, slots:, :] = rows_in[j]

    def wait_rows(d):
        for j in spots(d):
            all_columns(j, rows_in, ysend.at[0], yrecv.at[j]).wait_recv()

    def hop_sent(way, d):
        here = ring.at[way, pl.ds(plan.offset[d], plan.prefix[d]), :]
        remote(here, here, zsend.at[way, d - 1], zrecv.at[way, 0], ep=outward[way]).wait_send()

    def combine(d):
        wait_rows(d)
        for way, j in places(d):
            prepare(way, d, j)
        if d < H:
            for way in range(2):
                hop_sent(way, d + 1)

        def one(p, carry, joined):
            for way in range(2):
                if joined:
                    closer(way, d + 1, p).wait_recv()
                place = spread[way, pl.ds(pl.multiple_of(p * piece, piece), piece), :]
                mine = pl.ds(pl.multiple_of(plan.offset[d] + p * piece, piece), piece)
                for c in range(0, width, wide):
                    part = jnp.dot(
                        place, doubled[way, :, c : c + wide], preferred_element_type=jnp.float32
                    )
                    if joined:
                        there = pl.ds(pl.multiple_of(plan.offset[d + 1] + p * piece, piece), piece)
                        part = part + back[way, there, c : c + wide].astype(jnp.float32)
                    ring[way, mine, c : c + wide] = part.astype(jnp.bfloat16)
            for way in range(2):
                closer(way, d, p).start()
            return carry

        old, new = plan.pieces[d + 1], plan.pieces[d]
        if new > old:
            lax.fori_loop(old, new, functools.partial(one, joined=False), 0)
        if old:
            lax.fori_loop(0, old, functools.partial(one, joined=True), 0)

    def own_rows():
        wait_rows(0)
        prepare(0, 0, 0)
        for c in range(0, width, wide):
            gathered[:, c : c + wide] = jnp.dot(
                spread[0], doubled[0, :, c : c + wide], preferred_element_type=jnp.float32
            )
        for way in range(2):
            slot = iota((rows, rows), 0).astype(jnp.float32)
            rank = meta_ref[2, 4 + way : 5 + way, :]
            unsort[way] = jnp.where(slot == rank, 1.0, 0.0).T.astype(jnp.bfloat16)

    weights = []
    for i, (src, dst) in enumerate(((wg_ref, wg), (wu_ref, wu), (wd_ref, wd))):
        weights.append(remote(src, dst.at[1], wsend.at[i], wrecv.at[i], tp=other))
        weights.append(pltpu.make_async_copy(src, dst.at[0], wown.at[i]))
    for i, (kind, d, *which) in enumerate(schedule(plan)):
        if kind == "go":
            pass_on(d, *which)
        elif kind == "pick":
            pick_plane(d)
        elif kind == "expert":
            if d == 0:
                for copy in weights:
                    copy.wait()
            compute(d, *which)
        else:
            if d == 1:
                own_rows()
            combine(d)
        if i == 2:
            write(lead, rows)
            for copy in weights:
                copy.start()

    first, end = plan.offset[1], plan.offset[1] + rows
    early = end - piece
    for way in range(2):
        def arrive(p, carry, way=way):
            closer(way, 1, p).wait_recv()
            return carry

        lax.fori_loop(0, plan.pieces[1] - 1, arrive, 0)
    for c in range(0, width, wide):
        part = gathered[:, c : c + wide]
        for way in range(2):
            part = part + jnp.dot(
                unsort[way, :, : rows - piece], back[way, first:early, c : c + wide],
                preferred_element_type=jnp.float32,
            )
        gathered[:, c : c + wide] = part
    for way in range(2):
        closer(way, 1, plan.pieces[1] - 1).wait_recv()
    half_width, some = width // 2, rows // 2
    here = min(wide, half_width)

    def block(of, i):
        return out_ref.at[pl.ds(pl.multiple_of(of * rows + i * some, some), some), :]

    def swap(i, of):
        src = halves.at[other, pl.ds(i * some, some), :]
        return remote(src, block(of, i), fsend.at[i], frecv.at[i], tp=other)

    def put(i):
        return pltpu.make_async_copy(halves.at[core, pl.ds(i * some, some), :], block(core, i), osem.at[i])

    for i in range(2):
        part_rows = slice(i * some, (i + 1) * some)
        squares = jnp.zeros((some, 1), jnp.float32)
        for c in range(0, width, wide):
            part = gathered[part_rows, c : c + wide]
            for way in range(2):
                part = part + jnp.dot(
                    unsort[way, part_rows, rows - piece :], back[way, early:end, c : c + wide],
                    preferred_element_type=jnp.float32,
                )
            gathered[part_rows, c : c + wide] = part
            squares = squares + jnp.sum(part * part, axis=1, keepdims=True)
        inverse = lax.rsqrt(squares / width + EPS)
        for c in range(0, width, here):
            halves[c // half_width, part_rows, c % half_width : c % half_width + here] = (
                gathered[part_rows, c : c + here] * inverse
            ).astype(jnp.bfloat16)
        swap(i, core).start()
        put(i).start()

    sent = pl.ds(0, Z * (X - 1) // X)
    remote(stage.at[sent], stage.at[sent], xsend.at[0], xrecv.at[0], ep=outward[0]).wait_send()
    remote(arrived.at[sent], arrived.at[sent], ysend.at[0], yrecv.at[0], ep=outward[0]).wait_send()
    remote(metas, metas, msend.at[0], mrecv.at[0, 0], ep=outward[0]).wait_send()
    for way in range(2):
        hop_sent(way, 1)
        remote(
            ring.at[way], ring.at[way], bsend.at[way], zrecv.at[way, 0], ep=homeward[way]
        ).wait_send()
    for i in range(2):
        swap(i, core).wait_send()
        swap(i, other).wait_recv()
        put(i).wait()


def run_experts(plan, tokens, gain_in, expert_ids, gate_weights, w_gate, w_up, w_down):
    X, Z, H, rows, width = plan.X, plan.Z, plan.H, plan.rows, plan.width
    dma = pltpu.SemaphoreType.DMA
    bf16 = jnp.bfloat16
    return pl.pallas_call(
        functools.partial(experts_kernel, plan),
        out_shape=jax.ShapeDtypeStruct((2 * rows, width // 2), bf16),
        in_specs=[VMEM, VMEM, VMEM, VMEM, ANY, ANY, ANY],
        out_specs=ANY,
        scratch_shapes=[
            pltpu.VMEM((rows, width), bf16),
            pltpu.VMEM((rows, width), bf16),
            pltpu.VMEM((rows, width), bf16),
            pltpu.VMEM((3, 8, rows), jnp.float32),
            pltpu.VMEM((2, plan.total, width), bf16),
            pltpu.VMEM((2, plan.total, width), bf16),
            pltpu.VMEM((2, H, 8, rows), jnp.float32),
            pltpu.VMEM((Z, plan.slots, width), bf16),
            pltpu.VMEM((Z, plan.slots, width), bf16),
            pltpu.VMEM((Z, plan.slots, width), bf16),
            pltpu.VMEM((2, rows, 2 * plan.slots), bf16),
            pltpu.VMEM((2, 2 * plan.slots, width), bf16),
            pltpu.VMEM((2,) + w_gate.shape, bf16),
            pltpu.VMEM((2,) + w_up.shape, bf16),
            pltpu.VMEM((2,) + w_down.shape, bf16),
            pltpu.VMEM((2, rows, width // 2), bf16),
            pltpu.VMEM((2, rows, rows), bf16),
            pltpu.VMEM((2, rows, rows), bf16),
            pltpu.VMEM((rows, width), jnp.float32),
            dma((2, H)), dma((2, sum(plan.pieces) + plan.pieces[1])), dma((2,)), dma((1,)), dma((2, H)),
            dma((1,)), dma((Z,)), dma((1,)), dma((Z,)),
            dma((3,)), dma((3,)), dma((3,)), dma((2,)), dma((2,)), dma((2,)),
        ],
        compiler_params=pltpu.CompilerParams(
            collective_id=0, has_side_effects=True, vmem_limit_bytes=VMEM_LIMIT
        ),
        name="run_experts",
    )(
        tokens, gain_in.reshape(1, width), expert_ids.T, gate_weights.T,
        w_gate, w_up, w_down,
    )


CHUNKS = 4


def gain_kernel(scaled_ref, gain_ref, out_ref, came, goes, in_sem, out_sem):
    some = came.shape[1]

    def load(i):
        return pltpu.make_async_copy(scaled_ref.at[pl.ds(i * some, some), :], came.at[i], in_sem.at[i])

    def store(i):
        return pltpu.make_async_copy(goes.at[i], out_ref.at[pl.ds(i * some, some), :], out_sem.at[i])

    for i in range(CHUNKS):
        load(i).start()
    for i in range(CHUNKS):
        load(i).wait()
        goes[i] = (came[i].astype(jnp.float32) * gain_ref[...]).astype(jnp.bfloat16)
        store(i).start()
    for i in range(CHUNKS):
        store(i).wait()


def apply_gain(scaled, gain_out):
    rows, width = scaled.shape
    part = pltpu.VMEM((CHUNKS, rows // CHUNKS, width), scaled.dtype)
    dma = pltpu.SemaphoreType.DMA
    return pl.pallas_call(
        gain_kernel,
        out_shape=jax.ShapeDtypeStruct(scaled.shape, scaled.dtype),
        in_specs=[ANY, VMEM],
        out_specs=ANY,
        scratch_shapes=[part, part, dma((CHUNKS,)), dma((CHUNKS,))],
        name="apply_gain",
    )(scaled, gain_out.reshape(1, width))


def per_device(columns, tokens, gain_in, expert_ids, gate_weights, w_gate, w_up, w_down, gain_out):
    own_rows, width = tokens.shape
    members = lax.axis_size("ep")
    capacity = 2 * own_rows * expert_ids.shape[1] // members
    plan = Plan(own_rows, width, members, capacity, columns)
    scaled = run_experts(
        plan, tokens, gain_in, expert_ids, gate_weights, w_gate[0], w_up[0], w_down[0]
    )
    return apply_gain(scaled, gain_out)


def solution(mesh, columns=COLUMNS):
    placed = (
        P(("grp", "ep", "tp"), None),
        P(),
        P(("grp", "ep"), None),
        P(("grp", "ep"), None),
        P("ep", None, "tp"),
        P("ep", None, "tp"),
        P("ep", None, "tp"),
        P("tp"),
    )
    return jax.shard_map(
        functools.partial(per_device, columns),
        mesh=mesh, in_specs=placed, out_specs=P(("grp", "ep"), "tp"), check_vma=False,
    )
```

```python
import functools

import jax
import jax.numpy as jnp
from jax import lax
from jax.experimental import pallas as pl
from jax.experimental.pallas import tpu as pltpu
from jax.sharding import PartitionSpec as P

EPS = 1e-06
COLUMNS = 4
MESH = pl.DeviceIdType.MESH
VMEM = pl.BlockSpec(memory_space=pltpu.VMEM)
ANY = pl.BlockSpec(memory_space=pl.ANY)
VMEM_LIMIT = 60 * 1024 * 1024


class Plan:
    def __init__(self, rows, width, members, capacity, columns):
        self.rows, self.width, self.members, self.cap, self.X = rows, width, members, capacity, columns
        self.Z = members // columns
        self.H = self.Z // 2
        self.slots = columns * capacity
        self.piece = self.slots // 2
        self.prefix = [0] + [
            min(rows, (self.H - d) * self.slots + self.slots // 2) for d in range(1, self.H + 1)
        ] + [0]
        self.pieces = [n // self.piece for n in self.prefix]
        self.offset = [sum(self.prefix[:d]) for d in range(self.H + 2)]
        self.total = sum(self.prefix)
        self.most = max(self.pieces)

    def number(self, d, p):
        return self.offset[d] // self.piece + p

    def me(self):
        ep = lax.axis_index("ep")
        return ep // self.X, ep % self.X

    def at(self, z, x):
        return lax.rem(z + 2 * self.Z, self.Z) * self.X + lax.rem(x + 2 * self.X, self.X)


def remote(src, dst, send, recv, **where):
    return pltpu.make_async_remote_copy(
        src_ref=src, dst_ref=dst, send_sem=send, recv_sem=recv, device_id=where, device_id_type=MESH
    )


def greet(plan):
    z, x = plan.me()
    peers = [{"ep": plan.at(z + 1, x)}, {"ep": plan.at(z - 1, x)}]
    peers += [{"ep": plan.at(z, x + r)} for r in range(1, plan.X)]
    peers.append({"tp": 1 - lax.axis_index("tp")})
    barrier = pltpu.get_barrier_semaphore()
    for peer in peers:
        pl.semaphore_signal(barrier, inc=1, device_id=peer, device_id_type=MESH)
    return barrier, len(peers)


def iota(shape, dim):
    return lax.broadcasted_iota(jnp.int32, shape, dim)


def sort_tokens(plan, loading, x_ref, gain_ref, ids_ref, gates_ref, own, orders, meta_ref, normed):
    rows, X, Z, H = plan.rows, plan.X, plan.Z, plan.H
    z, _ = plan.me()
    mine = pl.ds(pl.multiple_of(lax.axis_index("tp") * rows, rows), rows)
    square = (rows, rows)
    sub, lane = iota(square, 0), iota(square, 1)
    eye = sub == lane

    def as_column(row):
        return jnp.sum(jnp.where(eye, row, 0.0), axis=1, keepdims=True)

    def count(mask, axis):
        return jnp.sum(jnp.where(mask, 1.0, 0.0), axis=axis, keepdims=True)

    rws = [ids_ref[k : k + 1, mine].astype(jnp.float32) for k in range(2)]
    cols = [as_column(r) for r in rws]
    grws = [gates_ref[k : k + 1, mine] for k in range(2)]
    gcols = [as_column(g) for g in grws]
    q_col, q_row, key_col, key_row = [], [], [[], []], [[], []]
    for k in range(2):
        slot_row = count((sub < lane) & (cols[0] == rws[k]), 0) + count((sub < lane) & (cols[1] == rws[k]), 0)
        slot_col = count((lane < sub) & (rws[0] == cols[k]), 1) + count((lane < sub) & (rws[1] == cols[k]), 1)
        q_row.append(rws[k] * plan.cap + slot_row)
        q_col.append(cols[k] * plan.cap + slot_col)
        for expert, keys in ((rws[k], key_row), (cols[k], key_col)):
            e = expert.astype(jnp.int32)
            ahead = e // X - z
            ahead = jnp.where(ahead < 0, ahead + Z, ahead)
            first = e % X < X // 2
            up = jnp.where((ahead < H) | ((ahead == H) & first), ahead, 0)
            down = jnp.where((ahead > H) | ((ahead == H) & ~first), Z - ahead, 0)
            keys[0].append(up.astype(jnp.float32))
            keys[1].append(down.astype(jnp.float32))
    for k in range(2):
        meta_ref[2, k : k + 1, :] = q_row[k]
        meta_ref[2, 2 + k : 3 + k, :] = grws[k]
    for way in range(2):
        far_col = jnp.maximum(*key_col[way])
        far_row = jnp.maximum(*key_row[way])
        rank_row = count((far_col > far_row) | ((far_col == far_row) & (sub < lane)), 0)
        rank_col = count((far_row > far_col) | ((far_row == far_col) & (lane < sub)), 1)
        meta_ref[2, 4 + way : 5 + way, :] = rank_row
        chosen = rank_col == lane.astype(jnp.float32)
        for k in range(2):
            meta_ref[way, k : k + 1, :] = jnp.sum(jnp.where(chosen, q_col[k], 0.0), axis=0, keepdims=True)
            meta_ref[way, 2 + k : 3 + k, :] = jnp.sum(jnp.where(chosen, gcols[k], 0.0), axis=0, keepdims=True)
        meta_ref[way, 4:8, :] = jnp.zeros((4, rows), jnp.float32)
        orders[way] = jnp.where(sub.astype(jnp.float32) == rank_row, 1.0, 0.0).astype(jnp.bfloat16)
    meta_ref[2, 6:8, :] = jnp.zeros((2, rows), jnp.float32)

    loading.wait()
    step = 32

    def norm_step(i, carry):
        here = pl.ds(pl.multiple_of(i * step, step), step)
        x = x_ref[here, :].astype(jnp.float32)
        scale = lax.rsqrt(jnp.mean(x * x, axis=1, keepdims=True) + EPS)
        normed[here, :] = (x * scale * gain_ref[...]).astype(jnp.bfloat16)
        return carry

    lax.fori_loop(0, rows // step, norm_step, 0)

    def write(lo, hi):
        n = min(512, plan.width)
        for way in range(2):
            for c in range(0, plan.width, n):
                own[way][lo:hi, c : c + n] = jnp.dot(
                    orders[way, lo:hi, :], normed[:, c : c + n], preferred_element_type=jnp.float32
                ).astype(jnp.bfloat16)

    return write


def hits(plan, meta, n, z, way, d, weighted):
    slots, cap = plan.slots, plan.cap
    slot = iota((slots, n), 0)
    base = z * slots
    total = jnp.zeros((slots, n), jnp.float32)
    for k in range(2):
        match = meta[k : k + 1, :n].astype(jnp.int32) - base == slot
        if d == plan.H:
            match = match & (slot < slots // 2 if way == 0 else slot >= slots // 2)
        total = total + jnp.where(match, meta[2 + k : 3 + k, :n] if weighted else 1.0, 0.0)
    return total


def schedule(plan):
    if plan.pieces != [0, 8, 8, 8, 8, 7, 5, 3, 1, 0]:
        raise ValueError("no schedule")

    def go(*pieces):
        return [("go", d, p) for d, p in pieces]

    def expert(d):
        return [("expert", d, 0), ("expert", d, 1)]

    def first(d):
        return go((d, 0), (d, 1), (d, 2))

    return (
        first(1) + [("pick", 0)] + first(2) + first(3) + first(4) + [("expert", 0, 0)]
        + first(5) + first(6) + first(7)
        + go((1, 3), (8, 0), (1, 4), (1, 5)) + [("pick", 7)]
        + go((2, 3), (2, 4), (1, 6)) + [("pick", 8)]
        + go((3, 3), (3, 4), (2, 5)) + [("expert", 7, 0)]
        + go((4, 3), (4, 4), (2, 6)) + [("expert", 7, 1)]
        + go((5, 3), (5, 4), (3, 5)) + [("expert", 8, 0)]
        + go((6, 3), (6, 4), (3, 6), (1, 7), (4, 5), (4, 6)) + [("pick", 6)]
        + go((2, 7), (5, 5), (5, 6)) + expert(6)
        + go((3, 7)) + [("sum", 8), ("pick", 5), ("sum", 7)]
        + go((4, 7)) + expert(5) + [("sum", 6), ("pick", 4), ("pick", 3), ("sum", 5)]
        + expert(4) + expert(3) + [("sum", 4), ("pick", 2), ("pick", 1)]
        + expert(2) + [("sum", 3)] + expert(1) + [("sum", 2), ("sum", 1)]
    )


def experts_kernel(
    plan,
    x_ref, gain_ref, ids_ref, gates_ref, wg_ref, wu_ref, wd_ref,
    out_ref,
    tokens, normed, plus_ref, minus_ref, meta_ref, ring, back, metas, stage, arrived, rows_in, spread, doubled,
    wg, wu, wd, halves, orders, unsort, gathered,
    zsend, zrecv, bsend, msend, mrecv, xsend, xrecv, ysend, yrecv,
    wsend, wrecv, wown, fsend, frecv, osem, tsem,
):
    X, Z, H, cap, piece = plan.X, plan.Z, plan.H, plan.cap, plan.piece
    rows, width, slots = plan.rows, plan.width, plan.slots
    wide = min(512, width)
    z, x = plan.me()
    core = lax.axis_index("tp")
    other = 1 - core
    loading = pltpu.make_async_copy(x_ref, tokens, tsem.at[0])
    loading.start()
    barrier, peers = greet(plan)
    own = (plus_ref, minus_ref)
    write = sort_tokens(
        plan, loading, tokens, gain_ref, ids_ref, gates_ref, own, orders, meta_ref, normed
    )
    lead = 3 * piece
    write(0, lead)
    pl.semaphore_wait(barrier, peers)

    outward = (plan.at(z + 1, x), plan.at(z - 1, x))
    homeward = (outward[1], outward[0])
    def places(d):
        if d == 0:
            return [(0, 0)]
        if d == H:
            return [(0, Z - 1), (1, Z - 1)]
        return [(0, 2 * d - 1), (1, 2 * d)]

    def spots(d):
        return sorted({j for _, j in places(d)})

    def passing(way, d, p):
        dst = ring.at[way, pl.ds(plan.offset[d] + p * piece, piece), :]
        if d == 1:
            src = own[way].at[pl.ds(p * piece, piece), :]
        else:
            src = ring.at[way, pl.ds(plan.offset[d - 1] + p * piece, piece), :]
        return remote(src, dst, zsend.at[way, d - 1], zrecv.at[way, plan.number(d, p)], ep=outward[way])

    def passing_meta(way, d):
        src = meta_ref.at[way] if d == 1 else metas.at[way, d - 2]
        return remote(src, metas.at[way, d - 1], msend.at[0], mrecv.at[way, d - 1], ep=outward[way])

    def back_sem(way, d, p):
        return zrecv.at[way, plan.number(d - 1, p) if d > 1 else sum(plan.pieces) + p]

    def closer(way, d, p):
        here = pl.ds(plan.offset[d] + p * piece, piece)
        return remote(
            ring.at[way, here, :], back.at[way, here, :],
            bsend.at[way], back_sem(way, d, p), ep=homeward[way],
        )

    def column(r):
        return pl.ds(pl.multiple_of(lax.rem(x + r, X) * cap, cap), cap)

    def hand_over(j, r):
        src, dst = stage.at[j, column(r), :], arrived.at[j, column(0), :]
        return remote(src, dst, xsend.at[0], xrecv.at[j], ep=plan.at(z, x + r))

    def give_back(j, r):
        src, dst = arrived.at[j, column(r), :], rows_in.at[j, column(0), :]
        return remote(src, dst, ysend.at[0], yrecv.at[j], ep=plan.at(z, x + r))

    def all_columns(j, ref, send, recv):
        part = ref.at[j, pl.ds(0, plan.slots - cap), :]
        return remote(part, part, send, recv, ep=plan.at(z, x + 1))

    def exchange(j, copy):
        for r in range(1, X):
            copy(j, r).start()
        if copy is hand_over:
            arrived[j, column(0), :] = stage[j, column(0), :]
        else:
            rows_in[j, column(0), :] = arrived[j, column(0), :]

    def pick(way, d, j):
        n = rows if d == 0 else plan.prefix[d]
        meta = meta_ref[0] if d == 0 else metas[way, d - 1]
        source = plus_ref if d == 0 else ring.at[way, pl.ds(plan.offset[d], n), :]
        chosen = hits(plan, meta, n, z, way, d, False).astype(jnp.bfloat16)

        def columns(c, carry):
            here = pl.ds(pl.multiple_of(c * wide, wide), wide)
            found = jnp.dot(chosen, source[:, here], preferred_element_type=jnp.float32)
            found = found.astype(jnp.bfloat16)
            if d == H:
                lo = way * (slots // 2)
                stage[j, lo : lo + slots // 2, here] = found[lo : lo + slots // 2, :]
            else:
                stage[j, :, here] = found
            return carry

        lax.fori_loop(0, width // wide, columns, 0)

    landed = set()

    def await_piece(d, p):
        if (d, p) not in landed:
            for way in range(2):
                passing(way, d, p).wait_recv()
            landed.add((d, p))

    def pass_on(d, p):
        for way in range(2):
            if p == 0 and d > 1:
                passing_meta(way, d - 1).wait_recv()
            if p == 0:
                passing_meta(way, d).start()
        if d > 1:
            await_piece(d - 1, p)
        for way in range(2):
            passing(way, d, p).start()

    def pick_plane(d):
        if d == H:
            for way in range(2):
                passing_meta(way, d).wait_recv()
        for p in range(plan.pieces[d]):
            await_piece(d, p)
        for way, j in places(d):
            pick(way, d, j)
        for j in spots(d):
            exchange(j, hand_over)

    def expert(j):
        hidden = []
        for half in range(2):
            gated = jnp.dot(arrived[j], wg[half], preferred_element_type=jnp.float32)
            upward = jnp.dot(arrived[j], wu[half], preferred_element_type=jnp.float32)
            hidden.append((gated / (1.0 + jnp.exp(-gated)) * upward).astype(jnp.bfloat16))
        step = min(256, width)

        def down(c, carry):
            here = pl.ds(pl.multiple_of(c * step, step), step)
            total = jnp.zeros((slots, step), jnp.float32)
            for half in range(2):
                part = lax.dot_general(
                    hidden[half], wd[half, here, :], (((1,), (1,)), ((), ())),
                    preferred_element_type=jnp.float32,
                )
                total = total + part.astype(jnp.bfloat16).astype(jnp.float32)
            arrived[j, :, here] = total.astype(jnp.bfloat16)
            return carry

        lax.fori_loop(0, width // step, down, 0)

    def compute(d, n):
        j = spots(d)[n]
        all_columns(j, arrived, xsend.at[0], xrecv.at[j]).wait_recv()
        expert(j)
        exchange(j, give_back)

    def prepare(way, d, j):
        n = rows if d == 0 else plan.prefix[d]
        meta = meta_ref[2] if d == 0 else metas[way, d - 1]
        w = hits(plan, meta, n, z, way, d, True)
        high = w.astype(jnp.bfloat16).astype(jnp.float32)
        spread[way, :n, :] = jnp.concatenate([high, w - high], axis=0).T.astype(jnp.bfloat16)
        doubled[way, :slots, :] = rows_in[j]
        doubled[way, slots:, :] = rows_in[j]

    def wait_rows(d):
        for j in spots(d):
            all_columns(j, rows_in, ysend.at[0], yrecv.at[j]).wait_recv()

    def hop_sent(way, d):
        here = ring.at[way, pl.ds(plan.offset[d], plan.prefix[d]), :]
        remote(here, here, zsend.at[way, d - 1], zrecv.at[way, 0], ep=outward[way]).wait_send()

    def combine(d):
        wait_rows(d)
        for way, j in places(d):
            prepare(way, d, j)
        if d < H:
            for way in range(2):
                hop_sent(way, d + 1)

        def one(p, carry, joined):
            for way in range(2):
                if joined:
                    closer(way, d + 1, p).wait_recv()
                place = spread[way, pl.ds(pl.multiple_of(p * piece, piece), piece), :]
                mine = pl.ds(pl.multiple_of(plan.offset[d] + p * piece, piece), piece)
                for c in range(0, width, wide):
                    part = jnp.dot(
                        place, doubled[way, :, c : c + wide], preferred_element_type=jnp.float32
                    )
                    if joined:
                        there = pl.ds(pl.multiple_of(plan.offset[d + 1] + p * piece, piece), piece)
                        part = part + back[way, there, c : c + wide].astype(jnp.float32)
                    ring[way, mine, c : c + wide] = part.astype(jnp.bfloat16)
            for way in range(2):
                closer(way, d, p).start()
            return carry

        old, new = plan.pieces[d + 1], plan.pieces[d]
        if new > old:
            lax.fori_loop(old, new, functools.partial(one, joined=False), 0)
        if old:
            lax.fori_loop(0, old, functools.partial(one, joined=True), 0)

    def own_rows():
        wait_rows(0)
        prepare(0, 0, 0)
        for c in range(0, width, wide):
            gathered[:, c : c + wide] = jnp.dot(
                spread[0], doubled[0, :, c : c + wide], preferred_element_type=jnp.float32
            )
        for way in range(2):
            slot = iota((rows, rows), 0).astype(jnp.float32)
            rank = meta_ref[2, 4 + way : 5 + way, :]
            unsort[way] = jnp.where(slot == rank, 1.0, 0.0).T.astype(jnp.bfloat16)

    weights = []
    for i, (src, dst) in enumerate(((wg_ref, wg), (wu_ref, wu), (wd_ref, wd))):
        weights.append(remote(src, dst.at[1], wsend.at[i], wrecv.at[i], tp=other))
        weights.append(pltpu.make_async_copy(src, dst.at[0], wown.at[i]))
    for i, (kind, d, *which) in enumerate(schedule(plan)):
        if kind == "go":
            pass_on(d, *which)
        elif kind == "pick":
            pick_plane(d)
        elif kind == "expert":
            if d == 0:
                for copy in weights:
                    copy.wait()
            compute(d, *which)
        else:
            if d == 1:
                own_rows()
            combine(d)
        if i == 2:
            write(lead, rows)
            for copy in weights:
                copy.start()

    first, end = plan.offset[1], plan.offset[1] + rows
    early = end - piece
    for way in range(2):
        def arrive(p, carry, way=way):
            closer(way, 1, p).wait_recv()
            return carry

        lax.fori_loop(0, plan.pieces[1] - 1, arrive, 0)
    for c in range(0, width, wide):
        part = gathered[:, c : c + wide]
        for way in range(2):
            part = part + jnp.dot(
                unsort[way, :, : rows - piece], back[way, first:early, c : c + wide],
                preferred_element_type=jnp.float32,
            )
        gathered[:, c : c + wide] = part
    for way in range(2):
        closer(way, 1, plan.pieces[1] - 1).wait_recv()
    half_width, parts = width // 2, 4
    some = rows // parts
    here = min(wide, half_width)

    def block(of, i):
        return out_ref.at[pl.ds(pl.multiple_of(of * rows + i * some, some), some), :]

    def swap(i, of):
        src = halves.at[other, pl.ds(i * some, some), :]
        return remote(src, block(of, i), fsend.at[i], frecv.at[i], tp=other)

    def put(i):
        return pltpu.make_async_copy(halves.at[core, pl.ds(i * some, some), :], block(core, i), osem.at[i])

    for i in range(parts):
        part_rows = slice(i * some, (i + 1) * some)
        squares = jnp.zeros((some, 1), jnp.float32)
        for c in range(0, width, wide):
            part = gathered[part_rows, c : c + wide]
            for way in range(2):
                part = part + jnp.dot(
                    unsort[way, part_rows, rows - piece :], back[way, early:end, c : c + wide],
                    preferred_element_type=jnp.float32,
                )
            gathered[part_rows, c : c + wide] = part
            squares = squares + jnp.sum(part * part, axis=1, keepdims=True)
        inverse = lax.rsqrt(squares / width + EPS)
        for c in range(0, width, here):
            halves[c // half_width, part_rows, c % half_width : c % half_width + here] = (
                gathered[part_rows, c : c + here] * inverse
            ).astype(jnp.bfloat16)
        swap(i, core).start()
        put(i).start()

    sent = pl.ds(0, Z * (X - 1) // X)
    remote(stage.at[sent], stage.at[sent], xsend.at[0], xrecv.at[0], ep=outward[0]).wait_send()
    remote(arrived.at[sent], arrived.at[sent], ysend.at[0], yrecv.at[0], ep=outward[0]).wait_send()
    remote(metas, metas, msend.at[0], mrecv.at[0, 0], ep=outward[0]).wait_send()
    for way in range(2):
        hop_sent(way, 1)
        remote(
            ring.at[way], ring.at[way], bsend.at[way], zrecv.at[way, 0], ep=homeward[way]
        ).wait_send()
    for i in range(parts):
        swap(i, core).wait_send()
        swap(i, other).wait_recv()
        put(i).wait()


def run_experts(plan, tokens, gain_in, expert_ids, gate_weights, w_gate, w_up, w_down):
    X, Z, H, rows, width = plan.X, plan.Z, plan.H, plan.rows, plan.width
    dma = pltpu.SemaphoreType.DMA
    bf16 = jnp.bfloat16
    return pl.pallas_call(
        functools.partial(experts_kernel, plan),
        out_shape=jax.ShapeDtypeStruct((2 * rows, width // 2), bf16),
        in_specs=[ANY, VMEM, VMEM, VMEM, ANY, ANY, ANY],
        out_specs=ANY,
        scratch_shapes=[
            pltpu.VMEM((rows, width), bf16),
            pltpu.VMEM((rows, width), bf16),
            pltpu.VMEM((rows, width), bf16),
            pltpu.VMEM((rows, width), bf16),
            pltpu.VMEM((3, 8, rows), jnp.float32),
            pltpu.VMEM((2, plan.total, width), bf16),
            pltpu.VMEM((2, plan.total, width), bf16),
            pltpu.VMEM((2, H, 8, rows), jnp.float32),
            pltpu.VMEM((Z, plan.slots, width), bf16),
            pltpu.VMEM((Z, plan.slots, width), bf16),
            pltpu.VMEM((Z, plan.slots, width), bf16),
            pltpu.VMEM((2, rows, 2 * plan.slots), bf16),
            pltpu.VMEM((2, 2 * plan.slots, width), bf16),
            pltpu.VMEM((2,) + w_gate.shape, bf16),
            pltpu.VMEM((2,) + w_up.shape, bf16),
            pltpu.VMEM((2,) + w_down.shape, bf16),
            pltpu.VMEM((2, rows, width // 2), bf16),
            pltpu.VMEM((2, rows, rows), bf16),
            pltpu.VMEM((2, rows, rows), bf16),
            pltpu.VMEM((rows, width), jnp.float32),
            dma((2, H)), dma((2, sum(plan.pieces) + plan.pieces[1])), dma((2,)), dma((1,)), dma((2, H)),
            dma((1,)), dma((Z,)), dma((1,)), dma((Z,)),
            dma((3,)), dma((3,)), dma((3,)), dma((4,)), dma((4,)), dma((4,)), dma((1,)),
        ],
        compiler_params=pltpu.CompilerParams(
            collective_id=0, has_side_effects=True, vmem_limit_bytes=VMEM_LIMIT
        ),
        name="run_experts",
    )(
        tokens, gain_in.reshape(1, width), expert_ids.T, gate_weights.T,
        w_gate, w_up, w_down,
    )


def per_device(columns, tokens, gain_in, expert_ids, gate_weights, w_gate, w_up, w_down, gain_out):
    own_rows, width = tokens.shape
    members = lax.axis_size("ep")
    capacity = 2 * own_rows * expert_ids.shape[1] // members
    plan = Plan(own_rows, width, members, capacity, columns)
    scaled = run_experts(
        plan, tokens, gain_in, expert_ids, gate_weights, w_gate[0], w_up[0], w_down[0]
    )
    return (scaled.astype(jnp.float32) * gain_out).astype(jnp.bfloat16)


def solution(mesh, columns=COLUMNS):
    placed = (
        P(("grp", "ep", "tp"), None),
        P(),
        P(("grp", "ep"), None),
        P(("grp", "ep"), None),
        P("ep", None, "tp"),
        P("ep", None, "tp"),
        P("ep", None, "tp"),
        P("tp"),
    )
    return jax.shard_map(
        functools.partial(per_device, columns),
        mesh=mesh, in_specs=placed, out_specs=P(("grp", "ep"), "tp"), check_vma=False,
    )
```
